128 devices in a mesh: rep: 2 (over z_hi), fs: 32 (over z_lo, y, x), tp: 2 (over core).
Axes of the slice: x: 4, y: 4, z: 4 (z_hi: 2, z_lo: 2; z = z_hi * 2 + z_lo), core: 2. Of those that a mesh axis runs over, the one named last changes fastest.
Arguments:
- tokens: bfloat16 [65536, 2048], P(('rep', 'fs')), may hold values from -6 to 6
- norm_mix: bfloat16 [2048], replicated, may hold values from 0.099609375 to 1.8984375
- w_unit: bfloat16 [2048, 1024], P('fs', 'tp'), may hold values from -0.125 to 0.125
- w_value: bfloat16 [2048, 1024], P('fs', 'tp'), may hold values from -0.125 to 0.125
- spatial: bfloat16 [4, 128, 128], replicated, may hold values from -0.52734375 to 0.52734375
- spatial_bias: bfloat16 [4, 128], replicated, may hold values from 0.099609375 to 1.8984375
- group_gain: bfloat16 [1024], replicated, may hold values from 0.099609375 to 1.8984375
- group_shift: bfloat16 [1024], replicated, may hold values from -3 to 3
- w_mix_out: bfloat16 [1024, 2048], P('tp', 'fs'), may hold values from -0.1875 to 0.1875
- norm_ffn: bfloat16 [2048], replicated, may hold values from 0.099609375 to 1.8984375
- w_gate: bfloat16 [2048, 2816], P('fs', 'tp'), may hold values from -0.125 to 0.125
- w_up: bfloat16 [2048, 2816], P('fs', 'tp'), may hold values from -0.125 to 0.125
- w_down: bfloat16 [2816, 2048], P('tp', 'fs'), may hold values from -0.109375 to 0.109375
Outputs:
- layer_out: bfloat16 [65536, 2048], P(('rep', 'fs', 'tp'))
The draws below stay inside these ranges and needn't reach their ends.
All inputs are finite; a program needn't handle non-finite values.
Results may differ from the reference program's by a relative error of at most 0.008.
Values may be sent and summed in bfloat16 or wider, within the bound.
No kernel may reach another device: no remote copies, remote signals or barrier semaphores. Data moves between devices by JAX's collectives and lax.ppermute only.
A program may use at most 128 MiB of HBM per device.

```python
import jax
import jax.numpy as jnp
from jax import lax

D = 2048
FF = 2816
GROUPS = 4
SPATIAL_WIDTH = 1024
BLOCK = 128
TOK_DEV = 1024
TOKENS = 65536


def shard_levels(key, shape, cuts, smallest, high):
    level, own = 1.0, jax.random.fold_in(key, 6)
    for dim, shards_of in cuts:
        steps = jnp.exp(jax.random.uniform(jax.random.fold_in(own, dim), (shards_of,), jnp.float32, smallest / len(cuts), high / len(cuts)))
        level = level * jnp.repeat(steps, shape[dim] // shards_of).reshape([-1 if axis == dim else 1 for axis in range(len(shape))])
    return level


def gaussian(stream_key, shape, scale, bound, split=(), held_as=jnp.bfloat16):
    values = jax.random.normal(stream_key, shape, jnp.float32) * scale
    if len(split) > 0:
        values = shard_levels(stream_key, shape, split, -0.22, 0.18) * values
    return jnp.clip(values, min=-bound, max=bound).astype(held_as)


def setup_inputs(seed: int = 0) -> dict:
    keys = jax.random.split(jax.random.key(seed), 14)
    return {
        "tokens": gaussian(keys[0], (TOKENS, D), 1.0, 6.0, ((0, 64),)),
        "norm_mix": jnp.clip(1.0 + 0.18 * jax.random.normal(keys[1], (D,), jnp.float32), 0.099609375, 1.8984375).astype(jnp.bfloat16),
        "w_unit": gaussian(keys[2], (D, SPATIAL_WIDTH), D ** -0.5, 0.125, ((0, 32), (1, 2))),
        "w_value": gaussian(keys[3], (D, SPATIAL_WIDTH), D ** -0.5, 0.125, ((0, 32), (1, 2))),
        "spatial": gaussian(keys[4], (GROUPS, BLOCK, BLOCK), (BLOCK ** -0.5), 0.52734375),
        "spatial_bias": jnp.clip(1.0 + 0.18 * jax.random.normal(keys[5], (GROUPS, BLOCK), jnp.float32), 0.099609375, 1.8984375).astype(jnp.bfloat16),
        "group_gain": jnp.clip(1.0 + 0.18 * jax.random.normal(keys[6], (SPATIAL_WIDTH,), jnp.float32), 0.099609375, 1.8984375).astype(jnp.bfloat16),
        "group_shift": gaussian(keys[7], (SPATIAL_WIDTH,), 0.5, 3.0),
        "w_mix_out": gaussian(keys[8], (SPATIAL_WIDTH, D), SPATIAL_WIDTH ** -0.5, 0.1875, ((0, 2), (1, 32))),
        "norm_ffn": jnp.clip(1.0 + 0.18 * jax.random.normal(keys[9], (D,), jnp.float32), 0.099609375, 1.8984375).astype(jnp.bfloat16),
        "w_gate": gaussian(keys[10], (D, FF), D ** -0.5, 0.125, ((0, 32), (1, 2))),
        "w_up": gaussian(keys[11], (D, FF), D ** -0.5, 0.125, ((0, 32), (1, 2))),
        "w_down": gaussian(keys[12], (FF, D), FF ** -0.5, 0.109375, ((0, 2), (1, 32))),
    }


def rms_scale(values, gain):
    values = values.astype(jnp.float32)
    scale = lax.rsqrt(lax.optimization_barrier(jnp.mean(values * values, axis=-1, keepdims=True)) + 1e-06)
    return values * scale * gain.astype(jnp.float32)

def spatial_unit(unit_pre, value_pre, spatial, spatial_bias, group_gain, group_shift):
    count, width = value_pre.shape
    groups = spatial.shape[0]
    block = spatial.shape[1]
    active = jax.nn.gelu(value_pre, approximate=True).reshape(count, groups, width // groups)
    center = lax.optimization_barrier(jnp.mean(active, axis=-1, keepdims=True))
    spread = lax.optimization_barrier(jnp.mean(jnp.square(active - center), axis=-1, keepdims=True))
    normal = ((active - center) * lax.rsqrt(spread + 1e-06)).reshape(count, width)
    normal = normal * group_gain.astype(jnp.float32) + group_shift.astype(jnp.float32)
    grouped = normal.astype(jnp.bfloat16)
    causal = jnp.tril(jnp.ones((block, block), dtype=bool))
    weights = jnp.where(causal[None], spatial, jnp.zeros_like(spatial))
    tiles = grouped.reshape(count // block, block, groups, width // groups)
    mixed = jnp.einsum('gts,nsgd->ntgd', weights.astype(jnp.float32), tiles.astype(jnp.float32))
    mixed = mixed + spatial_bias.astype(jnp.float32).T[None, :, :, None]
    return jax.nn.gelu(unit_pre, approximate=True) * mixed.reshape(count, width)

def reference(tokens, norm_mix, w_unit, w_value, spatial, spatial_bias, group_gain, group_shift, w_mix_out, norm_ffn, w_gate, w_up, w_down):

    def one_sequence(rows):
        normed = rms_scale(rows, norm_mix).astype(jnp.bfloat16)
        unit_pre = jnp.dot(normed, w_unit, preferred_element_type=jnp.float32)
        value_pre = jnp.dot(normed, w_value, preferred_element_type=jnp.float32)
        gated = spatial_unit(unit_pre, value_pre, spatial, spatial_bias, group_gain, group_shift).astype(jnp.bfloat16)
        h_mid = (rows.astype(jnp.float32) + jnp.dot(gated, w_mix_out, preferred_element_type=jnp.float32)).astype(jnp.bfloat16)
        normed_mid = rms_scale(h_mid, norm_ffn).astype(jnp.bfloat16)
        gate = jnp.dot(normed_mid, w_gate, preferred_element_type=jnp.float32)
        up = jnp.dot(normed_mid, w_up, preferred_element_type=jnp.float32)
        hidden = (jax.nn.silu(gate) * up).astype(jnp.bfloat16)
        return (h_mid.astype(jnp.float32) + jnp.dot(hidden, w_down, preferred_element_type=jnp.float32)).astype(jnp.bfloat16)
    sequences = tokens.reshape(-1, TOK_DEV, tokens.shape[1])
    return lax.map(one_sequence, sequences).reshape(tokens.shape)
```

```python
import jax
import jax.numpy as jnp
from jax import lax
from jax.sharding import PartitionSpec as P

EVERY = ("tp", "rep", "fs")


def rms_scale(values, gain):
    values = values.astype(jnp.float32)
    scale = lax.rsqrt(jnp.mean(values * values, axis=-1, keepdims=True) + 1e-06)
    return values * scale * gain.astype(jnp.float32)


def spatial_unit(unit_pre, value_pre, spatial, spatial_bias, group_gain, group_shift):
    count, width = value_pre.shape
    groups = spatial.shape[0]
    block = spatial.shape[1]
    active = jax.nn.gelu(value_pre, approximate=True).reshape(count, groups, width // groups)
    center = jnp.mean(active, axis=-1, keepdims=True)
    spread = jnp.mean(jnp.square(active - center), axis=-1, keepdims=True)
    normal = ((active - center) * lax.rsqrt(spread + 1e-06)).reshape(count, width)
    normal = normal * group_gain.astype(jnp.float32) + group_shift.astype(jnp.float32)
    grouped = normal.astype(jnp.bfloat16)
    causal = jnp.tril(jnp.ones((block, block), dtype=bool))
    weights = jnp.where(causal[None], spatial, jnp.zeros_like(spatial))
    tiles = grouped.reshape(count // block, block, groups, width // groups)
    mixed = jnp.einsum("gts,nsgd->ntgd", weights, tiles, preferred_element_type=jnp.float32)
    mixed = mixed + spatial_bias.astype(jnp.float32).T[None, :, :, None]
    return jax.nn.gelu(unit_pre, approximate=True) * mixed.reshape(count, width)


def dot_nt(a, b):
    return lax.dot_general(a, b, (((1,), (1,)), ((), ())), preferred_element_type=jnp.float32)


def dot_nn(a, b):
    return jnp.dot(a, b, preferred_element_type=jnp.float32)


def half_rows(x, part):
    size = x.shape[0] // 2
    return lax.dynamic_slice_in_dim(x, part * size, size, 0)


def in_rows(x):
    rep, fs, rows, k = x.shape
    return x.transpose(1, 0, 2, 3).reshape(fs * rep * rows, k)


def on_device(
    tokens, norm_mix, w_unit, w_value, spatial, spatial_bias, group_gain, group_shift,
    w_mix_out, norm_ffn, w_gate, w_up, w_down,
):
    rep = lax.axis_index("rep")
    reps, fs, tps = (lax.axis_size(a) for a in ("rep", "fs", "tp"))
    rows = tokens.shape[0] // tps
    mine = lax.dynamic_slice_in_dim(tokens, lax.axis_index("tp") * rows, rows, 0)

    first = jnp.concatenate(
        [jnp.where(rep == 0, w_unit, w_value), half_rows(w_mix_out.T, rep)], axis=0
    )
    second = jnp.concatenate(
        [jnp.where(rep == 0, w_gate, w_up), half_rows(w_down.T, rep)], axis=0
    )
    share = w_unit.shape[0]
    one = lax.all_gather(first, EVERY).reshape(tps, reps, fs, *first.shape)
    two = lax.all_gather(second, EVERY).reshape(tps, reps, fs, *second.shape)
    pre = one[:, :, :, :share].reshape(tps, reps, fs * share, -1)
    mid = two[:, :, :, :share].reshape(tps, reps, fs * share, -1)

    normed = rms_scale(mine, norm_mix).astype(jnp.bfloat16)
    unit_pre = jnp.concatenate([dot_nn(normed, pre[t, 0]) for t in range(tps)], axis=1)
    value_pre = jnp.concatenate([dot_nn(normed, pre[t, 1]) for t in range(tps)], axis=1)
    gated = spatial_unit(
        unit_pre, value_pre, spatial, spatial_bias, group_gain, group_shift
    ).astype(jnp.bfloat16)
    out_w = jnp.concatenate([in_rows(one[t, :, :, share:]) for t in range(tps)], axis=1)
    h_mid = (mine.astype(jnp.float32) + dot_nt(gated, out_w)).astype(jnp.bfloat16)
    normed_mid = rms_scale(h_mid, norm_ffn).astype(jnp.bfloat16)
    hidden = jnp.concatenate(
        [
            (jax.nn.silu(dot_nn(normed_mid, mid[t, 0])) * dot_nn(normed_mid, mid[t, 1])).astype(jnp.bfloat16)
            for t in range(tps)
        ],
        axis=1,
    )
    down = jnp.concatenate([in_rows(two[t, :, :, share:]) for t in range(tps)], axis=1)
    return (h_mid.astype(jnp.float32) + dot_nt(hidden, down)).astype(jnp.bfloat16)


def solution(mesh):
    placed = (
        P(("rep", "fs"), None), P(), P("fs", "tp"), P("fs", "tp"), P(), P(), P(), P(),
        P("tp", "fs"), P(), P("fs", "tp"), P("fs", "tp"), P("tp", "fs"),
    )
    return jax.shard_map(
        on_device, mesh=mesh, in_specs=placed, out_specs=P(("rep", "fs", "tp"), None), check_vma=False
    )
```

```python
import functools

import jax
import jax.numpy as jnp
from jax import lax
from jax.experimental import pallas as pl
from jax.experimental.pallas import tpu as pltpu
from jax.sharding import PartitionSpec as P

EVERY = ("tp", "rep", "fs")
CHIPS = ("rep", "fs")
RING = 4
BF16, F32 = jnp.bfloat16, jnp.float32
ANY = pl.BlockSpec(memory_space=pl.ANY)
VMEM = pl.BlockSpec(memory_space=pltpu.VMEM)


def shift(x, axis, by):
    pairs = []
    for z in range(RING):
        for y in range(RING):
            for c in range(RING):
                to = [z, y, c]
                to[axis] = (to[axis] + by) % RING
                pairs.append(((z * RING + y) * RING + c, (to[0] * RING + to[1]) * RING + to[2]))
    return lax.ppermute(x, CHIPS, pairs)


def direct_ring(x, axis):
    return [x, shift(x, axis, 1), shift(x, axis, 2), shift(x, axis, 3)]


def relayed_ring(x, axis):
    half = x.shape[0] // 2
    behind, ahead = shift(x, axis, 1), shift(x, axis, RING - 1)
    return x, behind, ahead, shift(behind[:half], axis, 1), shift(ahead[half:], axis, RING - 1)


def in_place(pieces, position):
    out = []
    for j in range(RING):
        q = (position - j) % RING
        piece = pieces[0]
        for k in range(1, RING):
            piece = jnp.where(q == k, pieces[k], piece)
        out.append(piece)
    return jnp.stack(out)


def rms_scale(values, gain):
    values = values.astype(F32)
    scale = lax.rsqrt(jnp.mean(values * values, axis=-1, keepdims=True) + 1e-06)
    return values * scale * gain.astype(F32)


def dot_nn(a, b):
    return jnp.dot(a, b, preferred_element_type=F32)


def dot_nt(a, b):
    return lax.dot_general(a, b, (((1,), (1,)), ((), ())), preferred_element_type=F32)


def gelu(x):
    return 0.5 * x * (1.0 + jnp.tanh(0.7978845608028654 * (x + 0.044715 * (x * x * x))))


def mixer_body(own, *refs):
    normed_hbm = refs[0]
    first, second = refs[1:6], refs[6:11]
    mask_w, bias, gain, shifts, out, rows, w_unit, w_value, w_out, sem_x, sem_u, sem_v, sem_o = refs[11:]
    tp, rep, fs = lax.axis_index("tp"), lax.axis_index("rep"), lax.axis_index("fs")
    z, y = 2 * rep + fs // 16, (fs // RING) % RING
    count = rows.shape[0]
    start = pl.multiple_of((tp if own else 1 - tp) * count, count)
    pltpu.make_async_copy(normed_hbm.at[pl.ds(start, count)], rows, sem_x).start()

    def place(ref, index, w, sem, group, at_z, at_y):
        line = (at_z % 2) * RING + at_y
        to = pl.multiple_of((at_z // 2) * 32, 32)
        pltpu.make_async_copy(ref.at[index, :, pl.ds(0, 32)], w.at[line, :, pl.ds(to, 32)], sem).start()
        to = pl.multiple_of((at_z // 2) * 32 + 16 * group, 16)
        pltpu.make_async_copy(ref.at[index, :, pl.ds(32, 16)], w_out.at[line, :, pl.ds(to, 16)], sem_o).start()

    for group, (pieces, w, sem) in enumerate(((first, w_unit, sem_u), (second, w_value, sem_v))):
        for piece, low, inner, outer in ((0, 0, 4, 0), (1, 0, 4, 1), (2, 0, 4, 3), (3, 0, 2, 2), (4, 2, 2, 2)):
            for i in range(inner):
                near = (low + i) % RING
                if group == 0:
                    at_z, at_y = (z + RING - outer) % RING, (y + RING - near) % RING
                else:
                    at_z, at_y = (z + RING - near) % RING, (y + RING - outer) % RING
                place(pieces[piece], i, w, sem, group, at_z, at_y)

    pltpu.make_async_copy(normed_hbm.at[pl.ds(start, count)], rows, sem_x).wait()
    pltpu.make_async_copy(w_value, w_value, sem_v).wait()
    x = rows[...]
    model, width = x.shape[1], w_value.shape[-1]
    value = gelu(dot_nn(x, w_value[...].reshape(model, width)))
    pltpu.make_async_copy(w_unit, w_unit, sem_u).wait()
    unit = gelu(dot_nn(x, w_unit[...].reshape(model, width)))
    groups, block = mask_w.shape[0], mask_w.shape[1]
    per = width // groups
    parts = []
    for g in range(groups):
        a = value[:, g * per : (g + 1) * per]
        a = a - jnp.mean(a, axis=-1, keepdims=True)
        a = a * lax.rsqrt(jnp.mean(a * a, axis=-1, keepdims=True) + 1e-06)
        a = a * gain[:, g * per : (g + 1) * per] + shifts[:, g * per : (g + 1) * per]
        a = a.astype(BF16)
        mixed = [
            dot_nn(mask_w[g], a[n * block : (n + 1) * block]) + bias[:, g : g + 1]
            for n in range(count // block)
        ]
        parts.append((unit[:, g * per : (g + 1) * per] * jnp.concatenate(mixed, axis=0)).astype(BF16))
    gated = jnp.concatenate(parts, axis=1)
    pltpu.make_async_copy(w_out, w_out, sem_o).wait()
    out[...] = dot_nt(gated, w_out[...].reshape(model, width)).astype(out.dtype)


def mixer(own, normed, first, second, mask_w, bias, gain, shifts, count, dtype):
    model, width = normed.shape[1], first[0].shape[-1]
    weight = pltpu.VMEM((8, RING, model // 32, width), BF16)
    return pl.pallas_call(
        functools.partial(mixer_body, own),
        out_shape=jax.ShapeDtypeStruct((count, model), dtype),
        in_specs=[ANY] * 11 + [VMEM] * 4,
        out_specs=VMEM,
        scratch_shapes=[pltpu.VMEM((count, model), BF16), weight, weight, weight] + [pltpu.SemaphoreType.DMA] * 4,
        compiler_params=pltpu.CompilerParams(vmem_limit_bytes=56 * 2**20),
        name="mixer_own" if own else "mixer_other",
    )(normed, *first, *second, mask_w, bias, gain, shifts)


CUTS = ((0, 512), (512, 512), (1024, 384))


def ffn_body(h_mid, normed, packed, out, gate, up, down, hidden, sem_w, sem_d):
    tps = gate.shape[0]
    wide = gate.shape[-1]
    share = gate.shape[2]
    count, model = out.shape

    def columns(t, c, w):
        low, size = CUTS[c]
        return pltpu.make_async_copy(
            packed.at[t, w, :, pl.ds(0, share), pl.ds(low, size)],
            (gate, up)[w].at[t, :, :, pl.ds(low, size)],
            sem_w.at[t, c, w],
        )

    def downs(t, r):
        half = share // 2
        return pltpu.make_async_copy(
            packed.at[t, r, :, pl.ds(share, half)], down.at[t, :, pl.ds(r * half, half)], sem_d.at[t, r]
        )

    steps = [(t, c) for t in range(tps) for c in range(len(CUTS))]
    for t, c in steps:
        columns(t, c, 0).start()
        columns(t, c, 1).start()
    for t in range(tps):
        downs(t, 0).start()
        downs(t, 1).start()
    x = normed[...]
    for t, c in steps:
        low, size = CUTS[c]
        columns(t, c, 0).wait()
        g = dot_nn(x, gate[t, :, :, low : low + size].reshape(model, size))
        columns(t, c, 1).wait()
        u = dot_nn(x, up[t, :, :, low : low + size].reshape(model, size))
        hidden[:, t * wide + low : t * wide + low + size] = (jax.nn.silu(g) * u).astype(BF16)
    for t in range(tps):
        downs(t, 0).wait()
        downs(t, 1).wait()
    chunk = 512
    lines = chunk // share
    for n in range(model // chunk):
        acc = h_mid[:, n * chunk : (n + 1) * chunk].astype(F32)
        for t in range(tps):
            w = down[t, n * lines : (n + 1) * lines].reshape(chunk, wide)
            acc = acc + dot_nt(hidden[:, t * wide : (t + 1) * wide], w)
        out[:, n * chunk : (n + 1) * chunk] = acc.astype(BF16)


def ffn(h_mid, normed, packed, share):
    tps, _, fs, _, wide = packed.shape
    whole = pltpu.VMEM((tps, fs, share, wide), BF16)
    return pl.pallas_call(
        ffn_body,
        out_shape=jax.ShapeDtypeStruct(h_mid.shape, BF16),
        in_specs=[VMEM, VMEM, ANY],
        out_specs=VMEM,
        scratch_shapes=[
            whole, whole, whole, pltpu.VMEM((h_mid.shape[0], tps * wide), BF16),
            pltpu.SemaphoreType.DMA((tps, len(CUTS), 2)), pltpu.SemaphoreType.DMA((tps, 2)),
        ],
        compiler_params=pltpu.CompilerParams(vmem_limit_bytes=58 * 2**20),
        name="ffn",
    )(h_mid, normed, packed)


def half_rows(x, part):
    size = x.shape[0] // 2
    return lax.dynamic_slice_in_dim(x, part * size, size, 0)


def on_device(
    tokens, norm_mix, w_unit, w_value, spatial, spatial_bias, group_gain, group_shift,
    w_mix_out, norm_ffn, w_gate, w_up, w_down,
):
    tp, rep, fs = (lax.axis_index(a) for a in ("tp", "rep", "fs"))
    tps, reps, fss = (lax.axis_size(a) for a in ("tp", "rep", "fs"))
    rows = tokens.shape[0] // tps
    share, width = w_unit.shape

    packed = jnp.concatenate([jnp.where(rep == 0, w_gate, w_up), half_rows(w_down.T, rep)], axis=0)
    packed = lax.all_gather(packed, EVERY).reshape(tps, reps, fss, *packed.shape)

    out_half = half_rows(w_mix_out.T, rep)
    mine = jnp.concatenate(
        [half_rows(w_unit, rep), out_half[:16], half_rows(w_value, rep), out_half[16:]], axis=0
    )
    line = in_place(direct_ring(mine, 2), fs % RING)
    cut = mine.shape[0] // 2
    first = relayed_ring(jnp.stack(direct_ring(line[:, :cut], 1)), 0)
    second = relayed_ring(jnp.stack(direct_ring(line[:, cut:], 0)), 1)

    groups = spatial.shape[0] // tps
    causal = jnp.tril(jnp.ones(spatial.shape[1:], dtype=bool))
    mask_w = lax.dynamic_slice_in_dim(jnp.where(causal[None], spatial, 0), tp * groups, groups, 0)
    bias = lax.dynamic_slice_in_dim(spatial_bias, tp * groups, groups, 0).astype(F32).T
    gain = lax.dynamic_slice_in_dim(group_gain, tp * width, width, 0).astype(F32)[None]
    shifts = lax.dynamic_slice_in_dim(group_shift, tp * width, width, 0).astype(F32)[None]
    normed = rms_scale(tokens, norm_mix).astype(BF16)

    unit = functools.partial(
        mixer, normed=normed, first=first, second=second, mask_w=mask_w, bias=bias, gain=gain,
        shifts=shifts, count=rows,
    )
    other = unit(False, dtype=BF16)
    arrived = lax.ppermute(other, "tp", [(i, (i + 1) % tps) for i in range(tps)])
    kept = unit(True, dtype=F32)
    residual = lax.dynamic_slice_in_dim(tokens, tp * rows, rows, 0).astype(F32)
    h_mid = (residual + (kept + arrived.astype(F32))).astype(BF16)
    normed_mid = rms_scale(h_mid, norm_ffn).astype(BF16)
    return ffn(h_mid, normed_mid, packed, share)


def solution(mesh):
    placed = (
        P(("rep", "fs"), None), P(), P("fs", "tp"), P("fs", "tp"), P(), P(), P(), P(),
        P("tp", "fs"), P(), P("fs", "tp"), P("fs", "tp"), P("tp", "fs"),
    )
    return jax.shard_map(
        on_device, mesh=mesh, in_specs=placed, out_specs=P(("rep", "fs", "tp"), None), check_vma=False
    )
```

```python
import functools

import jax
import jax.numpy as jnp
from jax import lax
from jax.experimental import pallas as pl
from jax.experimental.pallas import tpu as pltpu
from jax.sharding import PartitionSpec as P


EVERY = ("tp", "rep", "fs")
CHIPS = ("rep", "fs")
RING = 4
BF16, F32 = jnp.bfloat16, jnp.float32
ANY = pl.BlockSpec(memory_space=pl.ANY)
VMEM = pl.BlockSpec(memory_space=pltpu.VMEM)


def shift(x, axis, by):
    pairs = []
    for z in range(RING):
        for y in range(RING):
            for c in range(RING):
                to = [z, y, c]
                to[axis] = (to[axis] + by) % RING
                pairs.append(((z * RING + y) * RING + c, (to[0] * RING + to[1]) * RING + to[2]))
    return lax.ppermute(x, CHIPS, pairs)


def direct_ring(x, axis):
    return [x, shift(x, axis, 1), shift(x, axis, 2), shift(x, axis, 3)]


def relayed_ring(x, axis):
    half = x.shape[0] // 2
    behind, ahead = shift(x, axis, 1), shift(x, axis, RING - 1)
    return [x, behind, ahead, shift(behind[:half], axis, 1), shift(ahead[half:], axis, RING - 1)]


def in_place(pieces, position):
    out = []
    for j in range(RING):
        q = (position - j) % RING
        piece = pieces[0]
        for k in range(1, RING):
            piece = jnp.where(q == k, pieces[k], piece)
        out.append(piece)
    return jnp.stack(out)


def rms_scale(values, gain):
    values = values.astype(F32)
    scale = lax.rsqrt(jnp.mean(values * values, axis=-1, keepdims=True) + 1e-06)
    return values * scale * gain.astype(F32)


def dot_nn(a, b):
    return jnp.dot(a, b, preferred_element_type=F32)


def dot_nt(a, b):
    return lax.dot_general(a, b, (((1,), (1,)), ((), ())), preferred_element_type=F32)


def gelu(x):
    return 0.5 * x * (1.0 + jnp.tanh(0.7978845608028654 * (x + 0.044715 * (x * x * x))))


def mixer_body(own, *refs):
    normed_hbm = refs[0]
    first, second = refs[1:6], refs[6:11]
    mask_w, bias, gain, shifts, out, rows, w_unit, w_value, w_out, sem_x, sem_u, sem_v, sem_o = refs[11:]
    tp, rep, fs = lax.axis_index("tp"), lax.axis_index("rep"), lax.axis_index("fs")
    z, y = 2 * rep + fs // 16, (fs // RING) % RING
    count = rows.shape[0]
    start = pl.multiple_of((tp if own else 1 - tp) * count, count)
    pltpu.make_async_copy(normed_hbm.at[pl.ds(start, count)], rows, sem_x).start()

    def place(ref, index, w, sem, group, at_z, at_y):
        line = (at_z % 2) * RING + at_y
        to = pl.multiple_of((at_z // 2) * 32, 32)
        pltpu.make_async_copy(ref.at[index, :, pl.ds(0, 32)], w.at[line, :, pl.ds(to, 32)], sem).start()
        to = pl.multiple_of((at_z // 2) * 32 + 16 * group, 16)
        pltpu.make_async_copy(ref.at[index, :, pl.ds(32, 16)], w_out.at[line, :, pl.ds(to, 16)], sem_o).start()

    for group, (pieces, w, sem) in enumerate(((first, w_unit, sem_u), (second, w_value, sem_v))):
        for piece, low, inner, outer in ((0, 0, 4, 0), (1, 0, 4, 1), (2, 0, 4, 3), (3, 0, 2, 2), (4, 2, 2, 2)):
            for i in range(inner):
                near = (low + i) % RING
                if group == 0:
                    at_z, at_y = (z + RING - outer) % RING, (y + RING - near) % RING
                else:
                    at_z, at_y = (z + RING - near) % RING, (y + RING - outer) % RING
                place(pieces[piece], i, w, sem, group, at_z, at_y)

    pltpu.make_async_copy(normed_hbm.at[pl.ds(start, count)], rows, sem_x).wait()
    pltpu.make_async_copy(w_value, w_value, sem_v).wait()
    x = rows[...]
    model, width = x.shape[1], w_value.shape[-1]
    value = gelu(dot_nn(x, w_value[...].reshape(model, width)))
    pltpu.make_async_copy(w_unit, w_unit, sem_u).wait()
    unit = gelu(dot_nn(x, w_unit[...].reshape(model, width)))
    groups, block = mask_w.shape[0], mask_w.shape[1]
    per = width // groups
    parts = []
    for g in range(groups):
        a = value[:, g * per : (g + 1) * per]
        a = a - jnp.mean(a, axis=-1, keepdims=True)
        a = a * lax.rsqrt(jnp.mean(a * a, axis=-1, keepdims=True) + 1e-06)
        a = a * gain[:, g * per : (g + 1) * per] + shifts[:, g * per : (g + 1) * per]
        a = a.astype(BF16)
        mixed = [
            dot_nn(mask_w[g], a[n * block : (n + 1) * block]) + bias[:, g : g + 1]
            for n in range(count // block)
        ]
        parts.append((unit[:, g * per : (g + 1) * per] * jnp.concatenate(mixed, axis=0)).astype(BF16))
    gated = jnp.concatenate(parts, axis=1)
    pltpu.make_async_copy(w_out, w_out, sem_o).wait()
    out[...] = dot_nt(gated, w_out[...].reshape(model, width)).astype(out.dtype)


def mixer(own, normed, first, second, mask_w, bias, gain, shifts, count, dtype):
    model, width = normed.shape[1], first[0].shape[-1]
    weight = pltpu.VMEM((8, RING, model // 32, width), BF16)
    return pl.pallas_call(
        functools.partial(mixer_body, own),
        out_shape=jax.ShapeDtypeStruct((count, model), dtype),
        in_specs=[ANY] * 11 + [VMEM] * 4,
        out_specs=VMEM,
        scratch_shapes=[pltpu.VMEM((count, model), BF16), weight, weight, weight] + [pltpu.SemaphoreType.DMA] * 4,
        compiler_params=pltpu.CompilerParams(vmem_limit_bytes=56 * 2**20),
        name="mixer_own" if own else "mixer_other",
    )(normed, *first, *second, mask_w, bias, gain, shifts)


CUTS = ((0, 512), (512, 512), (1024, 384))


def ffn_body(*refs):
    tokens, kept, arrived, gain, packed = refs[:5]
    mine, theirs = refs[5:10], refs[10:15]
    out, rows, h_mid, normed, gate, up, down, hidden, sem_x, sem_w, sem_d = refs[15:]
    tp, rep, fs = lax.axis_index("tp"), lax.axis_index("rep"), lax.axis_index("fs")
    z, x = 2 * rep + fs // 16, fs % RING
    tps, wide, share = gate.shape[0], gate.shape[-1], gate.shape[2]
    count, model = out.shape
    start = pl.multiple_of(tp * count, count)
    residual = pltpu.make_async_copy(tokens.at[pl.ds(start, count)], rows, sem_x)

    def columns(t, c, w):
        low, size = CUTS[c]
        return pltpu.make_async_copy(
            packed.at[t, w, :, :, pl.ds(low, size)],
            (gate, up)[w].at[t, :, :, pl.ds(low, size)],
            sem_w.at[t, c, w],
        )

    steps = [(t, c) for t in range(tps) for c in range(len(CUTS))]
    residual.start()
    for t, c in steps:
        columns(t, c, 0).start()
        columns(t, c, 1).start()
    half = share // 2
    for pieces, t in ((mine, tp), (theirs, 1 - tp)):
        for piece, low, inner, outer in ((0, 0, 4, 0), (1, 0, 4, 1), (2, 0, 4, 3), (3, 0, 2, 2), (4, 2, 2, 2)):
            at_x = (x + RING - outer) % RING
            for i in range(inner):
                at_z = (z + RING - (low + i)) % RING
                to = pl.multiple_of((at_z // 2) * half, half)
                pltpu.make_async_copy(
                    pieces[piece].at[i], down.at[t, at_z % 2, :, at_x, pl.ds(to, half)], sem_d
                ).start()

    residual.wait()

    def prepare(r, carry):
        line = pl.ds(pl.multiple_of(r * 128, 128), 128)
        h = rows[line].astype(F32) + (kept[line] + arrived[line].astype(F32))
        h = h.astype(BF16)
        h_mid[line] = h
        h = h.astype(F32)
        scale = lax.rsqrt(jnp.mean(h * h, axis=-1, keepdims=True) + 1e-06)
        normed[line] = (h * scale * gain[...]).astype(BF16)
        return carry

    lax.fori_loop(0, count // 128, prepare, 0)
    n = normed[...]

    def wide_half(t, carry):
        for c in range(len(CUTS)):
            low, size = CUTS[c]
            columns(t, c, 0).wait()
            g = dot_nn(n, gate[t, :, :, low : low + size].reshape(model, size))
            columns(t, c, 1).wait()
            u = dot_nn(n, up[t, :, :, low : low + size].reshape(model, size))
            hidden[t, :, low : low + size] = (jax.nn.silu(g) * u).astype(BF16)
        return carry

    lax.fori_loop(0, tps, wide_half, 0)
    pltpu.make_async_copy(down, down, sem_d).wait()
    chunk = 512

    def columns_out(k, carry):
        cols = pl.ds(pl.multiple_of(k * chunk, chunk), chunk)
        acc = h_mid[:, cols].astype(F32)
        for t in range(tps):
            w = down[t, k // 2, pl.ds(2 * (k % 2), 2)].reshape(chunk, wide)
            acc = acc + dot_nt(hidden[t], w)
        out[:, cols] = acc.astype(BF16)
        return carry

    lax.fori_loop(0, model // chunk, columns_out, 0)


def ffn(tokens, kept, arrived, gain, packed, mine, theirs):
    tps, _, fs, share, wide = packed.shape
    count, model = kept.shape
    whole = pltpu.VMEM((tps, fs, share, wide), BF16)
    row = pltpu.VMEM((count, model), BF16)
    return pl.pallas_call(
        ffn_body,
        out_shape=jax.ShapeDtypeStruct((count, model), BF16),
        in_specs=[ANY, VMEM, VMEM, VMEM] + [ANY] * 11,
        out_specs=VMEM,
        scratch_shapes=[
            row, row, row, whole, whole,
            pltpu.VMEM((tps, 2, RING, RING, share, wide), BF16), pltpu.VMEM((tps, count, wide), BF16),
            pltpu.SemaphoreType.DMA, pltpu.SemaphoreType.DMA((tps, len(CUTS), 2)), pltpu.SemaphoreType.DMA,
        ],
        compiler_params=pltpu.CompilerParams(vmem_limit_bytes=60 * 2**20),
        name="ffn",
    )(tokens, kept, arrived, gain, packed, *mine, *theirs)


def half_rows(x, part):
    size = x.shape[0] // 2
    return lax.dynamic_slice_in_dim(x, part * size, size, 0)


def on_device(
    tokens, norm_mix, w_unit, w_value, spatial, spatial_bias, group_gain, group_shift,
    w_mix_out, norm_ffn, w_gate, w_up, w_down,
):
    tp, rep, fs = (lax.axis_index(a) for a in ("tp", "rep", "fs"))
    tps, reps, fss = (lax.axis_size(a) for a in ("tp", "rep", "fs"))
    rows = tokens.shape[0] // tps
    _, width = w_unit.shape

    packed = jnp.where(rep == 0, w_gate, w_up)
    packed = lax.all_gather(packed, EVERY).reshape(tps, reps, fss, *packed.shape)

    out_half = half_rows(w_mix_out.T, rep)
    mine = jnp.concatenate(
        [half_rows(w_unit, rep), out_half[:16], half_rows(w_value, rep), out_half[16:]], axis=0
    )
    line = direct_ring(mine, 2)
    line = in_place(line, fs % RING)
    cut = mine.shape[0] // 2
    first = direct_ring(line[:, :cut], 1)
    second = direct_ring(line[:, cut:], 0)
    first = relayed_ring(jnp.stack(first), 0)
    second = relayed_ring(jnp.stack(second), 1)

    down = half_rows(w_down.T, rep)
    down = direct_ring(down, 1)
    down = in_place(down, fs // RING % RING)
    down = direct_ring(down, 0)
    down = relayed_ring(jnp.stack(down), 2)

    groups = spatial.shape[0] // tps
    causal = jnp.tril(jnp.ones(spatial.shape[1:], dtype=bool))
    mask_w = lax.dynamic_slice_in_dim(jnp.where(causal[None], spatial, 0), tp * groups, groups, 0)
    bias = lax.dynamic_slice_in_dim(spatial_bias, tp * groups, groups, 0).astype(F32).T
    gain = lax.dynamic_slice_in_dim(group_gain, tp * width, width, 0).astype(F32)[None]
    shifts = lax.dynamic_slice_in_dim(group_shift, tp * width, width, 0).astype(F32)[None]
    normed = rms_scale(tokens, norm_mix).astype(BF16)

    unit = functools.partial(
        mixer, normed=normed, first=first, second=second, mask_w=mask_w, bias=bias, gain=gain,
        shifts=shifts, count=rows,
    )
    other = unit(False, dtype=BF16)
    swap = [(i, (i + 1) % tps) for i in range(tps)]
    arrived = lax.ppermute(other, "tp", swap)
    kept = unit(True, dtype=F32)
    kept, down[3], down[4] = lax.optimization_barrier((kept, down[3], down[4]))
    theirs = [lax.ppermute(piece, "tp", swap) for piece in down]
    gain = norm_ffn.astype(F32)[None]
    return ffn(tokens, kept, arrived, gain, packed, down, theirs)


def solution(mesh):
    placed = (
        P(("rep", "fs"), None), P(), P("fs", "tp"), P("fs", "tp"), P(), P(), P(), P(),
        P("tp", "fs"), P(), P("fs", "tp"), P("fs", "tp"), P("tp", "fs"),
    )

    return jax.shard_map(on_device, mesh=mesh, in_specs=placed, out_specs=P(("rep", "fs", "tp"), None), check_vma=False)
```

```python
import functools

import jax
import jax.numpy as jnp
from jax import lax
from jax.experimental import pallas as pl
from jax.experimental.pallas import tpu as pltpu
from jax.sharding import PartitionSpec as P


EVERY = ("tp", "rep", "fs")
CHIPS = ("rep", "fs")
RING = 4
BF16, F32 = jnp.bfloat16, jnp.float32
ANY = pl.BlockSpec(memory_space=pl.ANY)
VMEM = pl.BlockSpec(memory_space=pltpu.VMEM)


def shift(x, axis, by):
    pairs = []
    for z in range(RING):
        for y in range(RING):
            for c in range(RING):
                to = [z, y, c]
                to[axis] = (to[axis] + by) % RING
                pairs.append(((z * RING + y) * RING + c, (to[0] * RING + to[1]) * RING + to[2]))
    return lax.ppermute(x, CHIPS, pairs)


def direct_ring(x, axis):
    return [x, shift(x, axis, 1), shift(x, axis, 2), shift(x, axis, 3)]


def passed_ring(x, axis, by):
    behind, ahead = shift(x, axis, 1), shift(x, axis, RING - 1)
    far = shift(behind if by == 1 else ahead, axis, by % RING)
    return [x, behind, far, ahead]


def relayed_ring(x, axis):
    half = x.shape[0] // 2
    behind, ahead = shift(x, axis, 1), shift(x, axis, RING - 1)
    return [x, behind, ahead, shift(behind[:half], axis, 1), shift(ahead[half:], axis, RING - 1)]


RELAYED = ((0, 0, 4, 0), (1, 0, 4, 1), (2, 0, 4, 3), (3, 0, 2, 2), (4, 2, 2, 2))


def in_place(pieces, position):
    out = []
    for j in range(RING):
        q = (position - j) % RING
        piece = pieces[0]
        for k in range(1, RING):
            piece = jnp.where(q == k, pieces[k], piece)
        out.append(piece)
    return jnp.stack(out)


def rms_scale(values, gain):
    values = values.astype(F32)
    scale = lax.rsqrt(jnp.mean(values * values, axis=-1, keepdims=True) + 1e-06)
    return values * scale * gain.astype(F32)


def dot_nn(a, b):
    return jnp.dot(a, b, preferred_element_type=F32)


def dot_nt(a, b):
    return lax.dot_general(a, b, (((1,), (1,)), ((), ())), preferred_element_type=F32)


def gelu(x):
    return 0.5 * x * (1.0 + jnp.tanh(0.7978845608028654 * (x + 0.044715 * (x * x * x))))


def mixer_body(own, *refs):
    normed_hbm = refs[0]
    for_unit, for_value, for_out = refs[1:6], refs[6:11], refs[11:16]
    mask_w, bias, gain, shifts, out, rows, w_unit, w_value, w_out, sem_x, sem_u, sem_v, sem_o = refs[16:]
    tp, rep, fs = lax.axis_index("tp"), lax.axis_index("rep"), lax.axis_index("fs")
    z, y, x_at = 2 * rep + fs // 16, fs // RING % RING, fs % RING
    count = rows.shape[0]
    start = pl.multiple_of((tp if own else 1 - tp) * count, count)
    pltpu.make_async_copy(normed_hbm.at[pl.ds(start, count)], rows, sem_x).start()
    part = w_unit.shape[3] // 2

    def line(ref, index, w, sem, at_z, at_y):
        to = pl.ds(pl.multiple_of(at_z // 2 * part, part), part)
        pltpu.make_async_copy(ref.at[index], w.at[at_z % 2, at_y, :, to], sem).start()

    for piece, low, inner, outer in RELAYED:
        at_z, at_y = (z + RING - outer) % RING, (y + RING - outer) % RING

        def copies(i, carry, piece=piece, low=low, outer=outer):
            near_z, near_y = (z + RING - low - i) % RING, (y + RING - low - i) % RING
            line(for_value[piece], i, w_value, sem_v, near_z, at_y)
            line(for_unit[piece], i, w_unit, sem_u, at_z, near_y)
            for r in range(2):
                pltpu.make_async_copy(
                    for_out[piece].at[i, pl.ds(2 * r, 2)],
                    w_out.at[:, near_y, (x_at + RING - outer) % RING, pl.ds(r * part, part)],
                    sem_o,
                ).start()
            return carry

        lax.fori_loop(0, inner, copies, 0)

    pltpu.make_async_copy(normed_hbm.at[pl.ds(start, count)], rows, sem_x).wait()
    pltpu.make_async_copy(w_value, w_value, sem_v).wait()
    x = rows[...]
    model, width = x.shape[1], w_value.shape[-1]
    value = gelu(dot_nn(x, w_value[...].reshape(model, width)))
    pltpu.make_async_copy(w_unit, w_unit, sem_u).wait()
    unit = gelu(dot_nn(x, w_unit[...].reshape(model, width)))
    groups, block = mask_w.shape[0], mask_w.shape[1]
    per = width // groups
    parts = []
    for g in range(groups):
        a = value[:, g * per : (g + 1) * per]
        a = a - jnp.mean(a, axis=-1, keepdims=True)
        a = a * lax.rsqrt(jnp.mean(a * a, axis=-1, keepdims=True) + 1e-06)
        a = a * gain[:, g * per : (g + 1) * per] + shifts[:, g * per : (g + 1) * per]
        a = a.astype(BF16)
        mixed = [
            dot_nn(mask_w[g], a[n * block : (n + 1) * block]) + bias[:, g : g + 1]
            for n in range(count // block)
        ]
        parts.append((unit[:, g * per : (g + 1) * per] * jnp.concatenate(mixed, axis=0)).astype(BF16))
    gated = jnp.concatenate(parts, axis=1)
    pltpu.make_async_copy(w_out, w_out, sem_o).wait()
    out[...] = dot_nt(gated, w_out[...].reshape(model, width)).astype(out.dtype)


def mixer(own, normed, pieces, mask_w, bias, gain, shifts, count, dtype):
    model, width = normed.shape[1], pieces[0].shape[-1]
    weight = pltpu.VMEM((2, RING, RING, model // 32, width), BF16)
    return pl.pallas_call(
        functools.partial(mixer_body, own),
        out_shape=jax.ShapeDtypeStruct((count, model), dtype),
        in_specs=[ANY] * 16 + [VMEM] * 4,
        out_specs=VMEM,
        scratch_shapes=[pltpu.VMEM((count, model), BF16), weight, weight, weight] + [pltpu.SemaphoreType.DMA] * 4,
        compiler_params=pltpu.CompilerParams(vmem_limit_bytes=56 * 2**20),
        name="mixer_own" if own else "mixer_other",
    )(normed, *pieces, mask_w, bias, gain, shifts)


CHUNK = 512


def ffn_body(h_hbm, n_hbm, packed, out_hbm, h_mid, normed, mid, down, hidden, out, sem_h, sem_n, sem_w, sem_d, sem_o):
    tps, share, wide = packed.shape[0], down.shape[2], packed.shape[-1]
    _, model = out.shape
    starts = list(range(0, tps * wide, CHUNK))
    sizes = [min(CHUNK, tps * wide - at) for at in starts]

    def columns(j):
        copies = []
        for w in range(2):
            low, end = starts[j], starts[j] + sizes[j]
            while low < end:
                t = low // wide
                high = min(end, (t + 1) * wide)
                to = starts[j] + w * sizes[j] + low
                copies.append(
                    pltpu.make_async_copy(
                        packed.at[t, w, :, pl.ds(0, share), pl.ds(low - t * wide, high - low)],
                        mid.at[:, :, pl.ds(to, high - low)],
                        sem_w.at[j],
                    )
                )
                low = high
        return copies

    def downs(t):
        half = share // 2
        return [
            pltpu.make_async_copy(
                packed.at[t, r, :, pl.ds(share, half)], down.at[t, :, pl.ds(r * half, half)], sem_d
            )
            for r in range(2)
        ]

    rows = pltpu.make_async_copy(n_hbm, normed, sem_n)
    mids = pltpu.make_async_copy(h_hbm, h_mid, sem_h)
    rows.start()
    for j in range(len(sizes)):
        for copy in columns(j):
            copy.start()
    for t in range(tps):
        for copy in downs(t):
            copy.start()
    mids.start()
    rows.wait()

    def up_to(j, at, size):
        w = mid.at[:, :, pl.ds(2 * at, 2 * size)]
        pltpu.make_async_copy(w, w, sem_w.at[j]).wait()
        r = dot_nn(normed[...], w[...].reshape(model, 2 * size))
        hidden[:, pl.ds(at, size)] = (jax.nn.silu(r[:, :size]) * r[:, size:]).astype(BF16)

    def whole(j, carry):
        up_to(j, pl.multiple_of(j * CHUNK, CHUNK), CHUNK)
        return carry

    full = tps * wide // CHUNK
    lax.fori_loop(0, full, whole, 0)
    if full < len(sizes):
        up_to(full, starts[full], sizes[full])
    pltpu.make_async_copy(down, down, sem_d).wait()
    mids.wait()

    def leave(k):
        cols = pl.ds(pl.multiple_of(k * CHUNK, CHUNK), CHUNK)
        return pltpu.make_async_copy(out.at[:, cols], out_hbm.at[:, cols], sem_o.at[k])

    lines = CHUNK // share

    def back(k, carry):
        cols = pl.ds(pl.multiple_of(k * CHUNK, CHUNK), CHUNK)
        acc = h_mid[:, cols].astype(F32)
        for t in range(tps):
            w = down[t, pl.ds(k * lines, lines)].reshape(CHUNK, wide)
            acc = acc + dot_nt(hidden[:, t * wide : (t + 1) * wide], w)
        out[:, cols] = acc.astype(BF16)
        leave(k).start()
        return carry

    lax.fori_loop(0, model // CHUNK, back, 0)
    for k in range(model // CHUNK):
        leave(k).wait()


def ffn(h_mid, normed, packed, share):
    tps, _, fs, _, wide = packed.shape
    row = pltpu.VMEM(h_mid.shape, BF16)
    return pl.pallas_call(
        ffn_body,
        out_shape=jax.ShapeDtypeStruct(h_mid.shape, BF16),
        in_specs=[ANY] * 3,
        out_specs=ANY,
        scratch_shapes=[
            row, row, pltpu.VMEM((fs, share, 2 * tps * wide), BF16), pltpu.VMEM((tps, fs, share, wide), BF16),
            pltpu.VMEM((h_mid.shape[0], tps * wide), BF16), row,
            pltpu.SemaphoreType.DMA, pltpu.SemaphoreType.DMA, pltpu.SemaphoreType.DMA((-(-tps * wide // CHUNK),)),
            pltpu.SemaphoreType.DMA, pltpu.SemaphoreType.DMA((h_mid.shape[1] // CHUNK,)),
        ],
        compiler_params=pltpu.CompilerParams(vmem_limit_bytes=58 * 2**20),
        name="ffn",
    )(h_mid, normed, packed)


def half_rows(x, part):
    size = x.shape[0] // 2
    return lax.dynamic_slice_in_dim(x, part * size, size, 0)


def on_device(
    tokens, norm_mix, w_unit, w_value, spatial, spatial_bias, group_gain, group_shift,
    w_mix_out, norm_ffn, w_gate, w_up, w_down,
):
    tp, rep, fs = (lax.axis_index(a) for a in ("tp", "rep", "fs"))
    tps, reps, fss = (lax.axis_size(a) for a in ("tp", "rep", "fs"))
    rows = tokens.shape[0] // tps
    share, width = w_unit.shape

    packed = jnp.concatenate([jnp.where(rep == 0, w_gate, w_up), half_rows(w_down.T, rep)], axis=0)
    packed = lax.all_gather(packed, EVERY).reshape(tps, reps, fss, *packed.shape)

    part = share // 2
    line = jnp.concatenate([half_rows(w_unit, rep), half_rows(w_value, rep)], axis=0)
    line = in_place(direct_ring(line, 2), fs % RING)
    for_unit = relayed_ring(jnp.stack(passed_ring(line[:, :part], 1, 1)), 0)
    for_value = relayed_ring(jnp.stack(passed_ring(line[:, part:], 0, 1)), 1)
    for_out = in_place(direct_ring(half_rows(w_mix_out.T, rep), 0), 2 * rep + fs // 16)
    for_out = relayed_ring(jnp.stack(passed_ring(for_out, 1, -1)), 2)

    groups = spatial.shape[0] // tps
    causal = jnp.tril(jnp.ones(spatial.shape[1:], dtype=bool))
    mask_w = lax.dynamic_slice_in_dim(jnp.where(causal[None], spatial, 0), tp * groups, groups, 0)
    bias = lax.dynamic_slice_in_dim(spatial_bias, tp * groups, groups, 0).astype(F32).T
    gain = lax.dynamic_slice_in_dim(group_gain, tp * width, width, 0).astype(F32)[None]
    shifts = lax.dynamic_slice_in_dim(group_shift, tp * width, width, 0).astype(F32)[None]
    normed = rms_scale(tokens, norm_mix).astype(BF16)

    unit = functools.partial(
        mixer, normed=normed, pieces=(*for_unit, *for_value, *for_out), mask_w=mask_w, bias=bias, gain=gain,
        shifts=shifts, count=rows,
    )
    other = unit(False, dtype=BF16)
    arrived = lax.ppermute(other, "tp", [(i, (i + 1) % tps) for i in range(tps)])
    kept = unit(True, dtype=F32)
    residual = lax.dynamic_slice_in_dim(tokens, tp * rows, rows, 0).astype(F32)
    h_mid = (residual + (kept + arrived.astype(F32))).astype(BF16)
    normed_mid = rms_scale(h_mid, norm_ffn).astype(BF16)
    return ffn(h_mid, normed_mid, packed, share)


def solution(mesh):
    placed = (
        P(("rep", "fs"), None), P(), P("fs", "tp"), P("fs", "tp"), P(), P(), P(), P(),
        P("tp", "fs"), P(), P("fs", "tp"), P("fs", "tp"), P("tp", "fs"),
    )

    return jax.shard_map(on_device, mesh=mesh, in_specs=placed, out_specs=P(("rep", "fs", "tp"), None), check_vma=False)
```

```python
import functools

import jax
import jax.numpy as jnp
from jax import lax
from jax.experimental import pallas as pl
from jax.experimental.pallas import tpu as pltpu
from jax.sharding import PartitionSpec as P


EVERY = ("tp", "rep", "fs")
CHIPS = ("rep", "fs")
RING = 4
BF16, F32 = jnp.bfloat16, jnp.float32
ANY = pl.BlockSpec(memory_space=pl.ANY)
VMEM = pl.BlockSpec(memory_space=pltpu.VMEM)


def shift(x, axis, by):
    pairs = []
    for z in range(RING):
        for y in range(RING):
            for c in range(RING):
                to = [z, y, c]
                to[axis] = (to[axis] + by) % RING
                pairs.append(((z * RING + y) * RING + c, (to[0] * RING + to[1]) * RING + to[2]))
    return lax.ppermute(x, CHIPS, pairs)


def direct_ring(x, axis):
    return [x, shift(x, axis, 1), shift(x, axis, 2), shift(x, axis, 3)]


def passed_ring(x, axis, by):
    behind, ahead = shift(x, axis, 1), shift(x, axis, RING - 1)
    far = shift(behind if by == 1 else ahead, axis, by % RING)
    return [x, behind, far, ahead]


def relayed_ring(x, axis):
    half = x.shape[0] // 2
    behind, ahead = shift(x, axis, 1), shift(x, axis, RING - 1)
    return [x, behind, ahead, shift(behind[:half], axis, 1), shift(ahead[half:], axis, RING - 1)]


RELAYED = ((0, 0, 4, 0), (1, 0, 4, 1), (2, 0, 4, 3), (3, 0, 2, 2), (4, 2, 2, 2))


def in_place(pieces, position):
    out = []
    for j in range(RING):
        q = (position - j) % RING
        piece = pieces[0]
        for k in range(1, RING):
            piece = jnp.where(q == k, pieces[k], piece)
        out.append(piece)
    return jnp.stack(out)


def rms_scale(values, gain):
    values = values.astype(F32)
    scale = lax.rsqrt(jnp.mean(values * values, axis=-1, keepdims=True) + 1e-06)
    return values * scale * gain.astype(F32)


def dot_nn(a, b):
    return jnp.dot(a, b, preferred_element_type=F32)


def dot_nt(a, b):
    return lax.dot_general(a, b, (((1,), (1,)), ((), ())), preferred_element_type=F32)


def gelu(x):
    return 0.5 * x * (1.0 + jnp.tanh(0.7978845608028654 * (x + 0.044715 * (x * x * x))))


def mixer_body(own, *refs):
    normed_hbm = refs[0]
    for_unit, for_value, for_out = refs[1:6], refs[6:11], refs[11:16]
    mask_w, bias, gain, shifts, out, rows, w_unit, w_value, w_out, sem_x, sem_u, sem_v, sem_o = refs[16:]
    tp, rep, fs = lax.axis_index("tp"), lax.axis_index("rep"), lax.axis_index("fs")
    z, y, x_at = 2 * rep + fs // 16, fs // RING % RING, fs % RING
    count = rows.shape[0]
    start = pl.multiple_of((tp if own else 1 - tp) * count, count)
    pltpu.make_async_copy(normed_hbm.at[pl.ds(start, count)], rows, sem_x).start()
    part = w_unit.shape[3] // 2

    def line(ref, index, w, sem, at_z, at_y):
        to = pl.ds(pl.multiple_of(at_z // 2 * part, part), part)
        pltpu.make_async_copy(ref.at[index], w.at[at_z % 2, at_y, :, to], sem).start()

    for piece, low, inner, outer in RELAYED:
        at_z, at_y = (z + RING - outer) % RING, (y + RING - outer) % RING

        def copies(i, carry, piece=piece, low=low, outer=outer):
            near_z, near_y = (z + RING - low - i) % RING, (y + RING - low - i) % RING
            line(for_value[piece], i, w_value, sem_v, near_z, at_y)
            line(for_unit[piece], i, w_unit, sem_u, at_z, near_y)
            for r in range(2):
                pltpu.make_async_copy(
                    for_out[piece].at[i, pl.ds(2 * r, 2)],
                    w_out.at[:, near_y, (x_at + RING - outer) % RING, pl.ds(r * part, part)],
                    sem_o,
                ).start()
            return carry

        lax.fori_loop(0, inner, copies, 0)

    pltpu.make_async_copy(normed_hbm.at[pl.ds(start, count)], rows, sem_x).wait()
    pltpu.make_async_copy(w_value, w_value, sem_v).wait()
    x = rows[...]
    model, width = x.shape[1], w_value.shape[-1]
    value = gelu(dot_nn(x, w_value[...].reshape(model, width)))
    pltpu.make_async_copy(w_unit, w_unit, sem_u).wait()
    unit = gelu(dot_nn(x, w_unit[...].reshape(model, width)))
    groups, block = mask_w.shape[0], mask_w.shape[1]
    per = width // groups
    parts = []
    for g in range(groups):
        a = value[:, g * per : (g + 1) * per]
        a = a - jnp.mean(a, axis=-1, keepdims=True)
        a = a * lax.rsqrt(jnp.mean(a * a, axis=-1, keepdims=True) + 1e-06)
        a = a * gain[:, g * per : (g + 1) * per] + shifts[:, g * per : (g + 1) * per]
        a = a.astype(BF16)
        mixed = [
            dot_nn(mask_w[g], a[n * block : (n + 1) * block]) + bias[:, g : g + 1]
            for n in range(count // block)
        ]
        parts.append((unit[:, g * per : (g + 1) * per] * jnp.concatenate(mixed, axis=0)).astype(BF16))
    gated = jnp.concatenate(parts, axis=1)
    pltpu.make_async_copy(w_out, w_out, sem_o).wait()
    out[...] = dot_nt(gated, w_out[...].reshape(model, width)).astype(out.dtype)


def mixer(own, normed, pieces, mask_w, bias, gain, shifts, count, dtype):
    model, width = normed.shape[1], pieces[0].shape[-1]
    weight = pltpu.VMEM((2, RING, RING, model // 32, width), BF16)
    return pl.pallas_call(
        functools.partial(mixer_body, own),
        out_shape=jax.ShapeDtypeStruct((count, model), dtype),
        in_specs=[ANY] * 16 + [VMEM] * 4,
        out_specs=VMEM,
        scratch_shapes=[pltpu.VMEM((count, model), BF16), weight, weight, weight] + [pltpu.SemaphoreType.DMA] * 4,
        compiler_params=pltpu.CompilerParams(vmem_limit_bytes=56 * 2**20),
        name="mixer_own" if own else "mixer_other",
    )(normed, *pieces, mask_w, bias, gain, shifts)


CHUNK = 512


def ffn_body(h_hbm, n_hbm, packed, out_hbm, h_mid, normed, mid, down, hidden, out, sem_h, sem_n, sem_w, sem_d, sem_o):
    tps, share, wide = packed.shape[0], down.shape[2], packed.shape[-1]
    _, model = out.shape
    first = tps * wide % CHUNK
    starts = [0] * (first > 0) + list(range(first, tps * wide, CHUNK))
    sizes = [first] * (first > 0) + [CHUNK] * (tps * wide // CHUNK)

    def columns(j):
        copies = []
        for w in range(2):
            low, end = starts[j], starts[j] + sizes[j]
            while low < end:
                t = low // wide
                high = min(end, (t + 1) * wide)
                to = starts[j] + w * sizes[j] + low
                copies.append(
                    pltpu.make_async_copy(
                        packed.at[t, w, :, pl.ds(0, share), pl.ds(low - t * wide, high - low)],
                        mid.at[:, :, pl.ds(to, high - low)],
                        sem_w.at[j],
                    )
                )
                low = high
        return copies

    def downs(t):
        half = share // 2
        return [
            pltpu.make_async_copy(
                packed.at[t, r, :, pl.ds(share, half)], down.at[t, :, pl.ds(r * half, half)], sem_d
            )
            for r in range(2)
        ]

    rows = pltpu.make_async_copy(n_hbm, normed, sem_n)
    mids = pltpu.make_async_copy(h_hbm, h_mid, sem_h)
    for copy in columns(0):
        copy.start()
    rows.start()
    for j in range(1, len(sizes)):
        for copy in columns(j):
            copy.start()
    for t in range(tps):
        for copy in downs(t):
            copy.start()
    mids.start()
    rows.wait()

    def up_to(j, at, size):
        w = mid.at[:, :, pl.ds(2 * at, 2 * size)]
        pltpu.make_async_copy(w, w, sem_w.at[j]).wait()
        r = dot_nn(normed[...], w[...].reshape(model, 2 * size))
        hidden[:, pl.ds(at, size)] = (jax.nn.silu(r[:, :size]) * r[:, size:]).astype(BF16)

    if first:
        up_to(0, 0, first)

    def whole(j, carry):
        at = pl.multiple_of(first + j * CHUNK, 128)
        up_to(j + (first > 0), at, CHUNK)
        return carry

    lax.fori_loop(0, tps * wide // CHUNK, whole, 0)
    pltpu.make_async_copy(down, down, sem_d).wait()
    mids.wait()

    def leave(k):
        cols = pl.ds(pl.multiple_of(k * CHUNK, CHUNK), CHUNK)
        return pltpu.make_async_copy(out.at[:, cols], out_hbm.at[:, cols], sem_o.at[k])

    lines = CHUNK // share

    def back(k, carry):
        cols = pl.ds(pl.multiple_of(k * CHUNK, CHUNK), CHUNK)
        acc = h_mid[:, cols].astype(F32)
        for t in range(tps):
            w = down[t, pl.ds(k * lines, lines)].reshape(CHUNK, wide)
            acc = acc + dot_nt(hidden[:, t * wide : (t + 1) * wide], w)
        out[:, cols] = acc.astype(BF16)
        leave(k).start()
        return carry

    lax.fori_loop(0, model // CHUNK, back, 0)
    for k in range(model // CHUNK):
        leave(k).wait()


def ffn(h_mid, normed, packed, share):
    tps, _, fs, _, wide = packed.shape
    row = pltpu.VMEM(h_mid.shape, BF16)
    return pl.pallas_call(
        ffn_body,
        out_shape=jax.ShapeDtypeStruct(h_mid.shape, BF16),
        in_specs=[ANY] * 3,
        out_specs=ANY,
        scratch_shapes=[
            row, row, pltpu.VMEM((fs, share, 2 * tps * wide), BF16), pltpu.VMEM((tps, fs, share, wide), BF16),
            pltpu.VMEM((h_mid.shape[0], tps * wide), BF16), row,
            pltpu.SemaphoreType.DMA, pltpu.SemaphoreType.DMA, pltpu.SemaphoreType.DMA((-(-tps * wide // CHUNK),)),
            pltpu.SemaphoreType.DMA, pltpu.SemaphoreType.DMA((h_mid.shape[1] // CHUNK,)),
        ],
        compiler_params=pltpu.CompilerParams(vmem_limit_bytes=58 * 2**20),
        name="ffn",
    )(h_mid, normed, packed)


def pack_body(gate, up, down, out):
    rep = lax.axis_index("rep")
    share = gate.shape[0]
    half = share // 2
    out[:share] = jnp.where(rep == 0, gate[...], up[...])
    out[share:] = down[pl.ds(pl.multiple_of(rep * half, half), half)]


def pack(gate, up, down):
    share, wide = gate.shape
    return pl.pallas_call(
        pack_body,
        out_shape=jax.ShapeDtypeStruct((share + share // 2, wide), gate.dtype),
        in_specs=[VMEM] * 3,
        out_specs=VMEM,
        name="pack",
    )(gate, up, down)


def half_rows(x, part):
    size = x.shape[0] // 2
    return lax.dynamic_slice_in_dim(x, part * size, size, 0)


def on_device(
    tokens, norm_mix, w_unit, w_value, spatial, spatial_bias, group_gain, group_shift,
    w_mix_out, norm_ffn, w_gate, w_up, w_down,
):
    tp, rep, fs = (lax.axis_index(a) for a in ("tp", "rep", "fs"))
    tps, reps, fss = (lax.axis_size(a) for a in ("tp", "rep", "fs"))
    rows = tokens.shape[0] // tps
    share, width = w_unit.shape

    packed = pack(w_gate, w_up, w_down.T)
    packed = lax.all_gather(packed, EVERY).reshape(tps, reps, fss, *packed.shape)

    part = share // 2
    line = jnp.concatenate([half_rows(w_unit, rep), half_rows(w_value, rep)], axis=0)
    line = in_place(direct_ring(line, 2), fs % RING)
    for_unit = relayed_ring(jnp.stack(passed_ring(line[:, :part], 1, 1)), 0)
    for_value = relayed_ring(jnp.stack(passed_ring(line[:, part:], 0, 1)), 1)
    for_out = in_place(direct_ring(half_rows(w_mix_out.T, rep), 0), 2 * rep + fs // 16)
    for_out = relayed_ring(jnp.stack(passed_ring(for_out, 1, -1)), 2)

    groups = spatial.shape[0] // tps
    causal = jnp.tril(jnp.ones(spatial.shape[1:], dtype=bool))
    mask_w = lax.dynamic_slice_in_dim(jnp.where(causal[None], spatial, 0), tp * groups, groups, 0)
    bias = lax.dynamic_slice_in_dim(spatial_bias, tp * groups, groups, 0).astype(F32).T
    gain = lax.dynamic_slice_in_dim(group_gain, tp * width, width, 0).astype(F32)[None]
    shifts = lax.dynamic_slice_in_dim(group_shift, tp * width, width, 0).astype(F32)[None]
    normed = rms_scale(tokens, norm_mix).astype(BF16)

    unit = functools.partial(
        mixer, normed=normed, pieces=(*for_unit, *for_value, *for_out), mask_w=mask_w, bias=bias, gain=gain,
        shifts=shifts, count=rows,
    )
    other = unit(False, dtype=BF16)
    arrived = lax.ppermute(other, "tp", [(i, (i + 1) % tps) for i in range(tps)])
    kept = unit(True, dtype=F32)
    residual = lax.dynamic_slice_in_dim(tokens, tp * rows, rows, 0).astype(F32)
    h_mid = (residual + (kept + arrived.astype(F32))).astype(BF16)
    normed_mid = rms_scale(h_mid, norm_ffn).astype(BF16)
    return ffn(h_mid, normed_mid, packed, share)


def solution(mesh):
    placed = (
        P(("rep", "fs"), None), P(), P("fs", "tp"), P("fs", "tp"), P(), P(), P(), P(),
        P("tp", "fs"), P(), P("fs", "tp"), P("fs", "tp"), P("tp", "fs"),
    )

    return jax.shard_map(on_device, mesh=mesh, in_specs=placed, out_specs=P(("rep", "fs", "tp"), None), check_vma=False)
```

```python
import functools

import jax
import jax.numpy as jnp
from jax import lax
from jax.experimental import pallas as pl
from jax.experimental.pallas import tpu as pltpu
from jax.sharding import PartitionSpec as P


EVERY = ("tp", "rep", "fs")
CHIPS = ("rep", "fs")
RING = 4
BF16, F32 = jnp.bfloat16, jnp.float32
ANY = pl.BlockSpec(memory_space=pl.ANY)
VMEM = pl.BlockSpec(memory_space=pltpu.VMEM)


def shift(x, axis, by):
    pairs = []
    for z in range(RING):
        for y in range(RING):
            for c in range(RING):
                to = [z, y, c]
                to[axis] = (to[axis] + by) % RING
                pairs.append(((z * RING + y) * RING + c, (to[0] * RING + to[1]) * RING + to[2]))
    return lax.ppermute(x, CHIPS, pairs)


def direct_ring(x, axis):
    return [x, shift(x, axis, 1), shift(x, axis, 2), shift(x, axis, 3)]


def passed_ring(x, axis, by):
    behind, ahead = shift(x, axis, 1), shift(x, axis, RING - 1)
    far = shift(behind if by == 1 else ahead, axis, by % RING)
    return [x, behind, far, ahead]


def relayed_ring(x, axis):
    half = x.shape[0] // 2
    behind, ahead = shift(x, axis, 1), shift(x, axis, RING - 1)
    return [x, behind, ahead, shift(behind[:half], axis, 1), shift(ahead[half:], axis, RING - 1)]


RELAYED = ((0, 0, 4, 0), (1, 0, 4, 1), (2, 0, 4, 3), (3, 0, 2, 2), (4, 2, 2, 2))


def in_place(pieces, position):
    out = []
    for j in range(RING):
        q = (position - j) % RING
        piece = pieces[0]
        for k in range(1, RING):
            piece = jnp.where(q == k, pieces[k], piece)
        out.append(piece)
    return jnp.stack(out)


def rms_scale(values, gain):
    values = values.astype(F32)
    scale = lax.rsqrt(jnp.mean(values * values, axis=-1, keepdims=True) + 1e-06)
    return values * scale * gain.astype(F32)


def dot_nn(a, b):
    return jnp.dot(a, b, preferred_element_type=F32)


def dot_nt(a, b):
    return lax.dot_general(a, b, (((1,), (1,)), ((), ())), preferred_element_type=F32)


def gelu(x):
    return 0.5 * x * (1.0 + jnp.tanh(0.7978845608028654 * (x + 0.044715 * (x * x * x))))


def mixer_body(own, *refs):
    normed_hbm = refs[0]
    for_unit, for_value, for_out = refs[1:6], refs[6:11], refs[11:16]
    mask_w, bias, gain, shifts, out = refs[16:21]
    early = refs[21] if not own else None
    rows, w_unit, w_value, w_out, sem_x, sem_u, sem_v, sem_o, sem_e = refs[-9:]
    tp, rep, fs = lax.axis_index("tp"), lax.axis_index("rep"), lax.axis_index("fs")
    z, y, x_at = 2 * rep + fs // 16, fs // RING % RING, fs % RING
    count = rows.shape[0]
    start = pl.multiple_of((tp if own else 1 - tp) * count, count)
    pltpu.make_async_copy(normed_hbm.at[pl.ds(start, count)], rows, sem_x).start()
    part = w_unit.shape[3] // 2

    def line(ref, index, w, sem, at_z, at_y):
        to = pl.ds(pl.multiple_of(at_z // 2 * part, part), part)
        pltpu.make_async_copy(ref.at[index], w.at[at_z % 2, at_y, :, to], sem).start()

    def value_copies(piece, i, near, outer):
        line(for_value[piece], i, w_value, sem_v, (z + RING - near) % RING, (y + RING - outer) % RING)

    def unit_copies(piece, i, near, outer):
        line(for_unit[piece], i, w_unit, sem_u, (z + RING - outer) % RING, (y + RING - near) % RING)

    def out_copies(piece, i, near, outer):
        for r in range(2):
            pltpu.make_async_copy(
                for_out[piece].at[i, pl.ds(2 * r, 2)],
                w_out.at[:, (y + RING - near) % RING, (x_at + RING - outer) % RING, pl.ds(r * part, part)],
                sem_o,
            ).start()

    for start_copies in (value_copies, unit_copies, out_copies):
        for piece, low, inner, outer in RELAYED:

            def step(i, carry, piece=piece, low=low, outer=outer):
                start_copies(piece, i, low + i, outer)
                return carry

            lax.fori_loop(0, inner, step, 0)

    pltpu.make_async_copy(normed_hbm.at[pl.ds(start, count)], rows, sem_x).wait()
    pltpu.make_async_copy(w_value, w_value, sem_v).wait()
    x = rows[...]
    model, width = x.shape[1], gain.shape[-1]
    value = gelu(dot_nn(x, w_value[:, :, :, :, :width].reshape(model, width)))
    pltpu.make_async_copy(w_unit, w_unit, sem_u).wait()
    unit = gelu(dot_nn(x, w_unit[:, :, :, :, :width].reshape(model, width)))
    groups, block = mask_w.shape[0], mask_w.shape[1]
    per = width // groups
    parts = []
    for g in range(groups):
        a = value[:, g * per : (g + 1) * per]
        a = a - jnp.mean(a, axis=-1, keepdims=True)
        a = a * lax.rsqrt(jnp.mean(a * a, axis=-1, keepdims=True) + 1e-06)
        a = a * gain[:, g * per : (g + 1) * per] + shifts[:, g * per : (g + 1) * per]
        a = a.astype(BF16)
        mixed = [
            dot_nn(mask_w[g], a[n * block : (n + 1) * block]) + bias[:, g : g + 1]
            for n in range(count // block)
        ]
        parts.append((unit[:, g * per : (g + 1) * per] * jnp.concatenate(mixed, axis=0)).astype(BF16))
    gated = jnp.concatenate(parts, axis=1)
    pltpu.make_async_copy(w_out, w_out, sem_o).wait()
    hands = [] if own else [
        pltpu.make_async_copy(w.at[:, :, :, :, pl.ds(width, EARLY)], early.at[k], sem_e.at[k])
        for k, w in enumerate((w_unit, w_value, w_out))
    ]
    for hand in hands:
        hand.start()
    out[...] = dot_nt(gated, w_out[:, :, :, :, :width].reshape(model, width)).astype(out.dtype)
    for hand in hands:
        hand.wait()


def mixer(own, normed, pieces, mask_w, bias, gain, shifts, count, dtype):
    model, wide = normed.shape[1], pieces[0].shape[-1]
    lines = (2, RING, RING, model // 32)
    weight = pltpu.VMEM((*lines, wide), BF16)
    shape = jax.ShapeDtypeStruct((count, model), dtype)
    early = jax.ShapeDtypeStruct((3, *lines, EARLY), BF16)
    return pl.pallas_call(
        functools.partial(mixer_body, own),
        out_shape=shape if own else (shape, early),
        in_specs=[ANY] * 16 + [VMEM] * 4,
        out_specs=VMEM if own else (VMEM, ANY),
        scratch_shapes=[pltpu.VMEM((count, model), BF16), weight, weight, weight]
        + [pltpu.SemaphoreType.DMA] * 4 + [pltpu.SemaphoreType.DMA((3,))],
        compiler_params=pltpu.CompilerParams(vmem_limit_bytes=56 * 2**20),
        name="mixer_own" if own else "mixer_other",
    )(normed, *pieces, mask_w, bias, gain, shifts)


def early_body(tokens, kept_hbm, arrived_hbm, norm_gain, mine, theirs, acc, normed, rows, kept, arrived, mid, down, sem, sem_w, sem_d):
    tp = lax.axis_index("tp")
    count, model = rows.shape
    start = pl.multiple_of(tp * count, count)
    steps = count // 4
    ways = []
    for k in range(4):
        line = pl.ds(k * steps, steps)
        ways.append(
            [
                pltpu.make_async_copy(tokens.at[pl.ds(start + k * steps, steps)], rows.at[line], sem.at[k, 0]),
                pltpu.make_async_copy(kept_hbm.at[line], kept.at[line], sem.at[k, 1]),
                pltpu.make_async_copy(arrived_hbm.at[line], arrived.at[line], sem.at[k, 2]),
            ]
        )
    weights = [
        pltpu.make_async_copy(
            src.at[w], mid.at[:, :, :, :, pl.ds((2 * w + t) * EARLY, EARLY)], sem_w.at[w, t]
        )
        for t, src in enumerate((mine, theirs))
        for w in range(2)
    ]
    downs = [
        pltpu.make_async_copy(src.at[2], down.at[:, :, :, :, pl.ds(t * EARLY, EARLY)], sem_d.at[t])
        for t, src in enumerate((mine, theirs))
    ]
    for copies in (*ways, weights, downs):
        for copy in copies:
            copy.start()
    for k in range(4):
        line = slice(k * steps, (k + 1) * steps)
        for copy in ways[k]:
            copy.wait()
        h = rows[line].astype(F32) + (kept[line] + arrived[line].astype(F32))
        h = h.astype(BF16).astype(F32)
        kept[line] = h
        scale = lax.rsqrt(jnp.mean(h * h, axis=-1, keepdims=True) + 1e-06)
        normed[line] = (h * scale * norm_gain[...]).astype(BF16)
    for copy in weights:
        copy.wait()
    both = 2 * EARLY
    r = dot_nn(normed[...], mid[...].reshape(model, 2 * both))
    hidden = (jax.nn.silu(r[:, :both]) * r[:, both:]).astype(BF16)
    for copy in downs:
        copy.wait()
    acc[...] = kept[...] + dot_nt(hidden, down[...].reshape(model, both))


def early_units(tokens, kept, arrived, gain, mine, theirs):
    count, model = kept.shape
    lines = mine.shape[1:-1]
    row = pltpu.VMEM((count, model), BF16)
    return pl.pallas_call(
        early_body,
        out_shape=(jax.ShapeDtypeStruct((count, model), F32), jax.ShapeDtypeStruct((count, model), BF16)),
        in_specs=[ANY, ANY, ANY, VMEM, ANY, ANY],
        out_specs=(VMEM, VMEM),
        scratch_shapes=[
            row, pltpu.VMEM((count, model), F32), row,
            pltpu.VMEM((*lines, 4 * EARLY), BF16), pltpu.VMEM((*lines, 2 * EARLY), BF16),
            pltpu.SemaphoreType.DMA((4, 3)), pltpu.SemaphoreType.DMA((2, 2)), pltpu.SemaphoreType.DMA((2,)),
        ],
        compiler_params=pltpu.CompilerParams(vmem_limit_bytes=56 * 2**20),
        name="early_units",
    )(tokens, kept, arrived, gain, mine, theirs)


CHUNK = 512
EARLY = 128


def ffn_body(h_hbm, n_hbm, packed, out_hbm, h_mid, normed, mid, down, hidden, out, sem_h, sem_n, sem_w, sem_d, sem_o):
    tps, share, wide = packed.shape[0], down.shape[2], packed.shape[-1]
    _, model = out.shape
    first = tps * wide % CHUNK
    starts = [0] * (first > 0) + list(range(first, tps * wide, CHUNK))
    sizes = [first] * (first > 0) + [CHUNK] * (tps * wide // CHUNK)

    def columns(j):
        copies = []
        for w in range(2):
            low, end = starts[j], starts[j] + sizes[j]
            while low < end:
                t = low // wide
                high = min(end, (t + 1) * wide)
                to = starts[j] + w * sizes[j] + low
                copies.append(
                    pltpu.make_async_copy(
                        packed.at[t, w, :, pl.ds(0, share), pl.ds(low - t * wide, high - low)],
                        mid.at[:, :, pl.ds(to, high - low)],
                        sem_w.at[j],
                    )
                )
                low = high
        return copies

    def downs(t):
        half = share // 2
        return [
            pltpu.make_async_copy(
                packed.at[t, r, :, pl.ds(share, half)], down.at[t, :, pl.ds(r * half, half)], sem_d
            )
            for r in range(2)
        ]

    rows = pltpu.make_async_copy(n_hbm, normed, sem_n)
    mids = pltpu.make_async_copy(h_hbm, h_mid, sem_h)
    for copy in columns(0):
        copy.start()
    rows.start()
    for j in range(1, len(sizes)):
        for copy in columns(j):
            copy.start()
    for t in range(tps):
        for copy in downs(t):
            copy.start()
    mids.start()
    rows.wait()

    def up_to(j, at, size):
        w = mid.at[:, :, pl.ds(2 * at, 2 * size)]
        pltpu.make_async_copy(w, w, sem_w.at[j]).wait()
        r = dot_nn(normed[...], w[...].reshape(model, 2 * size))
        hidden[:, pl.ds(at, size)] = (jax.nn.silu(r[:, :size]) * r[:, size:]).astype(BF16)

    if first:
        up_to(0, 0, first)

    def whole(j, carry):
        at = pl.multiple_of(first + j * CHUNK, 128)
        up_to(j + (first > 0), at, CHUNK)
        return carry

    lax.fori_loop(0, tps * wide // CHUNK, whole, 0)
    pltpu.make_async_copy(down, down, sem_d).wait()
    mids.wait()

    def leave(k):
        cols = pl.ds(pl.multiple_of(k * CHUNK, CHUNK), CHUNK)
        return pltpu.make_async_copy(out.at[:, cols], out_hbm.at[:, cols], sem_o.at[k])

    lines = CHUNK // share

    def back(k, carry):
        cols = pl.ds(pl.multiple_of(k * CHUNK, CHUNK), CHUNK)
        acc = h_mid[:, cols]
        for t in range(tps):
            w = down[t, pl.ds(k * lines, lines)].reshape(CHUNK, wide)
            acc = acc + dot_nt(hidden[:, t * wide : (t + 1) * wide], w)
        out[:, cols] = acc.astype(BF16)
        leave(k).start()
        return carry

    lax.fori_loop(0, model // CHUNK, back, 0)
    for k in range(model // CHUNK):
        leave(k).wait()


def ffn(h_mid, normed, packed, share):
    tps, _, fs, _, wide = packed.shape
    row = pltpu.VMEM(h_mid.shape, BF16)
    return pl.pallas_call(
        ffn_body,
        out_shape=jax.ShapeDtypeStruct(h_mid.shape, BF16),
        in_specs=[ANY] * 3,
        out_specs=ANY,
        scratch_shapes=[
            pltpu.VMEM(h_mid.shape, F32), row, pltpu.VMEM((fs, share, 2 * tps * wide), BF16), pltpu.VMEM((tps, fs, share, wide), BF16),
            pltpu.VMEM((h_mid.shape[0], tps * wide), BF16), row,
            pltpu.SemaphoreType.DMA, pltpu.SemaphoreType.DMA, pltpu.SemaphoreType.DMA((-(-tps * wide // CHUNK),)),
            pltpu.SemaphoreType.DMA, pltpu.SemaphoreType.DMA((h_mid.shape[1] // CHUNK,)),
        ],
        compiler_params=pltpu.CompilerParams(vmem_limit_bytes=58 * 2**20),
        name="ffn",
    )(h_mid, normed, packed)


def pack_body(gate, up, down, out):
    rep = lax.axis_index("rep")
    share = gate.shape[0]
    half = share // 2
    out[:share] = jnp.where(rep == 0, gate[:, EARLY:], up[:, EARLY:])
    out[share:] = down[pl.ds(pl.multiple_of(rep * half, half), half), EARLY:]


def pack(gate, up, down):
    share, wide = gate.shape
    return pl.pallas_call(
        pack_body,
        out_shape=jax.ShapeDtypeStruct((share + share // 2, wide - EARLY), gate.dtype),
        in_specs=[VMEM] * 3,
        out_specs=VMEM,
        name="pack",
    )(gate, up, down)


def half_rows(x, part):
    size = x.shape[0] // 2
    return lax.dynamic_slice_in_dim(x, part * size, size, 0)


def on_device(
    tokens, norm_mix, w_unit, w_value, spatial, spatial_bias, group_gain, group_shift,
    w_mix_out, norm_ffn, w_gate, w_up, w_down,
):
    tp, rep, fs = (lax.axis_index(a) for a in ("tp", "rep", "fs"))
    tps, reps, fss = (lax.axis_size(a) for a in ("tp", "rep", "fs"))
    rows = tokens.shape[0] // tps
    share, width = w_unit.shape

    packed = pack(w_gate, w_up, w_down.T)
    packed = lax.all_gather(packed, EVERY).reshape(tps, reps, fss, *packed.shape)

    part = share // 2

    def beside(w, extra):
        return jnp.concatenate([half_rows(w, rep), half_rows(extra[:, :EARLY], rep)], axis=1)

    line = jnp.concatenate([beside(w_unit, w_gate), beside(w_value, w_up)], axis=0)
    line = in_place(direct_ring(line, 2), fs % RING)
    for_unit = relayed_ring(jnp.stack(passed_ring(line[:, :part], 1, 1)), 0)
    for_value = relayed_ring(jnp.stack(passed_ring(line[:, part:], 0, 1)), 1)
    for_out = beside(w_mix_out.T, w_down.T)
    for_out = in_place(direct_ring(for_out, 0), 2 * rep + fs // 16)
    for_out = relayed_ring(jnp.stack(passed_ring(for_out, 1, -1)), 2)

    groups = spatial.shape[0] // tps
    causal = jnp.tril(jnp.ones(spatial.shape[1:], dtype=bool))
    mask_w = lax.dynamic_slice_in_dim(jnp.where(causal[None], spatial, 0), tp * groups, groups, 0)
    bias = lax.dynamic_slice_in_dim(spatial_bias, tp * groups, groups, 0).astype(F32).T
    gain = lax.dynamic_slice_in_dim(group_gain, tp * width, width, 0).astype(F32)[None]
    shifts = lax.dynamic_slice_in_dim(group_shift, tp * width, width, 0).astype(F32)[None]
    normed = rms_scale(tokens, norm_mix).astype(BF16)

    unit = functools.partial(
        mixer, normed=normed, pieces=(*for_unit, *for_value, *for_out), mask_w=mask_w, bias=bias, gain=gain,
        shifts=shifts, count=rows,
    )
    other, early = unit(False, dtype=BF16)
    swap = [(i, (i + 1) % tps) for i in range(tps)]
    arrived = lax.ppermute(other, "tp", swap)
    early_theirs = lax.ppermute(early, "tp", swap)
    kept = unit(True, dtype=F32)
    gain = norm_ffn.astype(F32)[None]
    acc, normed_mid = early_units(tokens, kept, arrived, gain, early, early_theirs)
    return ffn(acc, normed_mid, packed, share)


def solution(mesh):
    placed = (
        P(("rep", "fs"), None), P(), P("fs", "tp"), P("fs", "tp"), P(), P(), P(), P(),
        P("tp", "fs"), P(), P("fs", "tp"), P("fs", "tp"), P("tp", "fs"),
    )

    return jax.shard_map(on_device, mesh=mesh, in_specs=placed, out_specs=P(("rep", "fs", "tp"), None), check_vma=False)
```

```python
import functools

import jax
import jax.numpy as jnp
from jax import lax
from jax.experimental import pallas as pl
from jax.experimental.pallas import tpu as pltpu
from jax.sharding import PartitionSpec as P


EVERY = ("tp", "rep", "fs")
CHIPS = ("rep", "fs")
RING = 4
BF16, F32 = jnp.bfloat16, jnp.float32
ANY = pl.BlockSpec(memory_space=pl.ANY)
VMEM = pl.BlockSpec(memory_space=pltpu.VMEM)


def shift(x, axis, by):
    pairs = []
    for z in range(RING):
        for y in range(RING):
            for c in range(RING):
                to = [z, y, c]
                to[axis] = (to[axis] + by) % RING
                pairs.append(((z * RING + y) * RING + c, (to[0] * RING + to[1]) * RING + to[2]))
    return lax.ppermute(x, CHIPS, pairs)


def direct_ring(x, axis):
    return [x, shift(x, axis, 1), shift(x, axis, 2), shift(x, axis, 3)]


def passed_ring(x, axis, by):
    behind, ahead = shift(x, axis, 1), shift(x, axis, RING - 1)
    far = shift(behind if by == 1 else ahead, axis, by % RING)
    return [x, behind, far, ahead]


def relayed_ring(x, axis):
    half = x.shape[0] // 2
    behind, ahead = shift(x, axis, 1), shift(x, axis, RING - 1)
    return [x, behind, ahead, shift(behind[:half], axis, 1), shift(ahead[half:], axis, RING - 1)]


RELAYED = ((0, 0, 4, 0), (1, 0, 4, 1), (2, 0, 4, 3), (3, 0, 2, 2), (4, 2, 2, 2))


def in_place(pieces, position):
    out = []
    for j in range(RING):
        q = (position - j) % RING
        piece = pieces[0]
        for k in range(1, RING):
            piece = jnp.where(q == k, pieces[k], piece)
        out.append(piece)
    return jnp.stack(out)


def rms_scale(values, gain):
    values = values.astype(F32)
    scale = lax.rsqrt(jnp.mean(values * values, axis=-1, keepdims=True) + 1e-06)
    return values * scale * gain.astype(F32)


def dot_nn(a, b):
    return jnp.dot(a, b, preferred_element_type=F32)


def dot_nt(a, b):
    return lax.dot_general(a, b, (((1,), (1,)), ((), ())), preferred_element_type=F32)


def gelu(x):
    return 0.5 * x * (1.0 + jnp.tanh(0.7978845608028654 * (x + 0.044715 * (x * x * x))))


def mixer_body(own, *refs):
    normed_hbm = refs[0]
    for_unit, for_value, for_out = refs[1:6], refs[6:11], refs[11:16]
    mask_w, bias, gain, shifts, out, rows, w_unit, w_value, w_out, sem_x, sem_u, sem_v, sem_o = refs[16:]
    tp, rep, fs = lax.axis_index("tp"), lax.axis_index("rep"), lax.axis_index("fs")
    z, y, x_at = 2 * rep + fs // 16, fs // RING % RING, fs % RING
    count = rows.shape[0]
    start = pl.multiple_of((tp if own else 1 - tp) * count, count)
    pltpu.make_async_copy(normed_hbm.at[pl.ds(start, count)], rows, sem_x).start()
    part = w_unit.shape[3] // 2

    def line(ref, index, w, sem, at_z, at_y):
        to = pl.ds(pl.multiple_of(at_z // 2 * part, part), part)
        pltpu.make_async_copy(ref.at[index], w.at[at_z % 2, at_y, :, to], sem).start()

    def value_copies(piece, i, near, outer):
        line(for_value[piece], i, w_value, sem_v, (z + RING - near) % RING, (y + RING - outer) % RING)

    def unit_copies(piece, i, near, outer):
        line(for_unit[piece], i, w_unit, sem_u, (z + RING - outer) % RING, (y + RING - near) % RING)

    def out_copies(piece, i, near, outer):
        for r in range(2):
            pltpu.make_async_copy(
                for_out[piece].at[i, pl.ds(2 * r, 2)],
                w_out.at[:, (y + RING - near) % RING, (x_at + RING - outer) % RING, pl.ds(r * part, part)],
                sem_o,
            ).start()

    for start_copies in (value_copies, unit_copies, out_copies):
        for piece, low, inner, outer in RELAYED:

            def step(i, carry, piece=piece, low=low, outer=outer):
                start_copies(piece, i, low + i, outer)
                return carry

            lax.fori_loop(0, inner, step, 0)

    pltpu.make_async_copy(normed_hbm.at[pl.ds(start, count)], rows, sem_x).wait()
    pltpu.make_async_copy(w_value, w_value, sem_v).wait()
    x = rows[...]
    model, width = x.shape[1], w_value.shape[-1]
    value = gelu(dot_nn(x, w_value[...].reshape(model, width)))
    pltpu.make_async_copy(w_unit, w_unit, sem_u).wait()
    unit = gelu(dot_nn(x, w_unit[...].reshape(model, width)))
    groups, block = mask_w.shape[0], mask_w.shape[1]
    per = width // groups
    parts = []
    for g in range(groups):
        a = value[:, g * per : (g + 1) * per]
        a = a - jnp.mean(a, axis=-1, keepdims=True)
        a = a * lax.rsqrt(jnp.mean(a * a, axis=-1, keepdims=True) + 1e-06)
        a = a * gain[:, g * per : (g + 1) * per] + shifts[:, g * per : (g + 1) * per]
        a = a.astype(BF16)
        mixed = [
            dot_nn(mask_w[g], a[n * block : (n + 1) * block]) + bias[:, g : g + 1]
            for n in range(count // block)
        ]
        parts.append((unit[:, g * per : (g + 1) * per] * jnp.concatenate(mixed, axis=0)).astype(BF16))
    gated = jnp.concatenate(parts, axis=1)
    pltpu.make_async_copy(w_out, w_out, sem_o).wait()
    out[...] = dot_nt(gated, w_out[...].reshape(model, width)).astype(out.dtype)


def mixer(own, normed, pieces, mask_w, bias, gain, shifts, count, dtype):
    model, width = normed.shape[1], pieces[0].shape[-1]
    weight = pltpu.VMEM((2, RING, RING, model // 32, width), BF16)
    return pl.pallas_call(
        functools.partial(mixer_body, own),
        out_shape=jax.ShapeDtypeStruct((count, model), dtype),
        in_specs=[ANY] * 16 + [VMEM] * 4,
        out_specs=VMEM,
        scratch_shapes=[pltpu.VMEM((count, model), BF16), weight, weight, weight] + [pltpu.SemaphoreType.DMA] * 4,
        compiler_params=pltpu.CompilerParams(vmem_limit_bytes=56 * 2**20),
        name="mixer_own" if own else "mixer_other",
    )(normed, *pieces, mask_w, bias, gain, shifts)


CHUNK = 512


def ffn_body(h_hbm, n_hbm, packed, out_hbm, h_mid, normed, mid, down, hidden, out, sem_h, sem_n, sem_w, sem_d, sem_o):
    tps, share, wide = packed.shape[0], down.shape[2], packed.shape[-1]
    _, model = out.shape
    first = tps * wide % CHUNK
    starts = [0] * (first > 0) + list(range(first, tps * wide, CHUNK))
    sizes = [first] * (first > 0) + [CHUNK] * (tps * wide // CHUNK)

    def columns(j):
        copies = []
        for w in range(2):
            low, end = starts[j], starts[j] + sizes[j]
            while low < end:
                t = low // wide
                high = min(end, (t + 1) * wide)
                to = starts[j] + w * sizes[j] + low
                copies.append(
                    pltpu.make_async_copy(
                        packed.at[t, w, :, pl.ds(0, share), pl.ds(low - t * wide, high - low)],
                        mid.at[:, :, pl.ds(to, high - low)],
                        sem_w.at[j],
                    )
                )
                low = high
        return copies

    def downs(t):
        half = share // 2
        return [
            pltpu.make_async_copy(
                packed.at[t, r, :, pl.ds(share, half)], down.at[t, :, pl.ds(r * half, half)], sem_d
            )
            for r in range(2)
        ]

    rows = pltpu.make_async_copy(n_hbm, normed, sem_n)
    mids = pltpu.make_async_copy(h_hbm, h_mid, sem_h)
    for copy in columns(0):
        copy.start()
    rows.start()
    for j in range(1, len(sizes)):
        for copy in columns(j):
            copy.start()
    for t in range(tps):
        for copy in downs(t):
            copy.start()
    mids.start()
    rows.wait()

    def up_to(j, at, size):
        w = mid.at[:, :, pl.ds(2 * at, 2 * size)]
        pltpu.make_async_copy(w, w, sem_w.at[j]).wait()
        r = dot_nn(normed[...], w[...].reshape(model, 2 * size))
        hidden[:, pl.ds(at, size)] = (jax.nn.silu(r[:, :size]) * r[:, size:]).astype(BF16)

    if first:
        up_to(0, 0, first)

    def whole(j, carry):
        at = pl.multiple_of(first + j * CHUNK, 128)
        up_to(j + (first > 0), at, CHUNK)
        return carry

    lax.fori_loop(0, tps * wide // CHUNK, whole, 0)
    pltpu.make_async_copy(down, down, sem_d).wait()
    mids.wait()

    def leave(k):
        cols = pl.ds(pl.multiple_of(k * CHUNK, CHUNK), CHUNK)
        return pltpu.make_async_copy(out.at[:, cols], out_hbm.at[:, cols], sem_o.at[k])

    lines = CHUNK // share

    def back(k, carry):
        cols = pl.ds(pl.multiple_of(k * CHUNK, CHUNK), CHUNK)
        acc = h_mid[:, cols].astype(F32)
        for t in range(tps):
            w = down[t, pl.ds(k * lines, lines)].reshape(CHUNK, wide)
            acc = acc + dot_nt(hidden[:, t * wide : (t + 1) * wide], w)
        out[:, cols] = acc.astype(BF16)
        leave(k).start()
        return carry

    lax.fori_loop(0, model // CHUNK, back, 0)
    for k in range(model // CHUNK):
        leave(k).wait()


def ffn(h_mid, normed, packed, share):
    tps, _, fs, _, wide = packed.shape
    row = pltpu.VMEM(h_mid.shape, BF16)
    return pl.pallas_call(
        ffn_body,
        out_shape=jax.ShapeDtypeStruct(h_mid.shape, BF16),
        in_specs=[ANY] * 3,
        out_specs=ANY,
        scratch_shapes=[
            row, row, pltpu.VMEM((fs, share, 2 * tps * wide), BF16), pltpu.VMEM((tps, fs, share, wide), BF16),
            pltpu.VMEM((h_mid.shape[0], tps * wide), BF16), row,
            pltpu.SemaphoreType.DMA, pltpu.SemaphoreType.DMA, pltpu.SemaphoreType.DMA((-(-tps * wide // CHUNK),)),
            pltpu.SemaphoreType.DMA, pltpu.SemaphoreType.DMA((h_mid.shape[1] // CHUNK,)),
        ],
        compiler_params=pltpu.CompilerParams(vmem_limit_bytes=58 * 2**20),
        name="ffn",
    )(h_mid, normed, packed)


def pack_body(gate, up, down, out):
    rep = lax.axis_index("rep")
    share = gate.shape[0]
    half = share // 2
    out[:share] = jnp.where(rep == 0, gate[...], up[...])
    out[share:] = down[pl.ds(pl.multiple_of(rep * half, half), half)]


def pack(gate, up, down):
    share, wide = gate.shape
    return pl.pallas_call(
        pack_body,
        out_shape=jax.ShapeDtypeStruct((share + share // 2, wide), gate.dtype),
        in_specs=[VMEM] * 3,
        out_specs=VMEM,
        name="pack",
    )(gate, up, down)


def half_rows(x, part):
    size = x.shape[0] // 2
    return lax.dynamic_slice_in_dim(x, part * size, size, 0)


def on_device(
    tokens, norm_mix, w_unit, w_value, spatial, spatial_bias, group_gain, group_shift,
    w_mix_out, norm_ffn, w_gate, w_up, w_down,
):
    tp, rep, fs = (lax.axis_index(a) for a in ("tp", "rep", "fs"))
    tps, reps, fss = (lax.axis_size(a) for a in ("tp", "rep", "fs"))
    rows = tokens.shape[0] // tps
    share, width = w_unit.shape

    packed = pack(w_gate, w_up, w_down.T)
    packed = lax.all_gather(packed, EVERY).reshape(tps, reps, fss, *packed.shape)

    part = share // 2
    line = jnp.concatenate([half_rows(w_unit, rep), half_rows(w_value, rep)], axis=0)
    line = in_place(direct_ring(line, 2), fs % RING)
    for_unit = relayed_ring(jnp.stack(passed_ring(line[:, :part], 1, 1)), 0)
    for_value = relayed_ring(jnp.stack(passed_ring(line[:, part:], 0, 1)), 1)
    for_out = in_place(direct_ring(half_rows(w_mix_out.T, rep), 0), 2 * rep + fs // 16)
    for_out = relayed_ring(jnp.stack(passed_ring(for_out, 1, -1)), 2)

    groups = spatial.shape[0] // tps
    causal = jnp.tril(jnp.ones(spatial.shape[1:], dtype=bool))
    mask_w = lax.dynamic_slice_in_dim(jnp.where(causal[None], spatial, 0), tp * groups, groups, 0)
    bias = lax.dynamic_slice_in_dim(spatial_bias, tp * groups, groups, 0).astype(F32).T
    gain = lax.dynamic_slice_in_dim(group_gain, tp * width, width, 0).astype(F32)[None]
    shifts = lax.dynamic_slice_in_dim(group_shift, tp * width, width, 0).astype(F32)[None]
    normed = rms_scale(tokens, norm_mix).astype(BF16)

    unit = functools.partial(
        mixer, normed=normed, pieces=(*for_unit, *for_value, *for_out), mask_w=mask_w, bias=bias, gain=gain,
        shifts=shifts, count=rows,
    )
    other = unit(False, dtype=BF16)
    arrived = lax.ppermute(other, "tp", [(i, (i + 1) % tps) for i in range(tps)])
    kept = unit(True, dtype=F32)
    residual = lax.dynamic_slice_in_dim(tokens, tp * rows, rows, 0).astype(F32)
    h_mid = (residual + (kept + arrived.astype(F32))).astype(BF16)
    normed_mid = rms_scale(h_mid, norm_ffn).astype(BF16)
    return ffn(h_mid, normed_mid, packed, share)


def solution(mesh):
    placed = (
        P(("rep", "fs"), None), P(), P("fs", "tp"), P("fs", "tp"), P(), P(), P(), P(),
        P("tp", "fs"), P(), P("fs", "tp"), P("fs", "tp"), P("tp", "fs"),
    )

    return jax.shard_map(on_device, mesh=mesh, in_specs=placed, out_specs=P(("rep", "fs", "tp"), None), check_vma=False)
```

```python
import functools

import jax
import jax.numpy as jnp
from jax import lax
from jax.experimental import pallas as pl
from jax.experimental.pallas import tpu as pltpu
from jax.sharding import PartitionSpec as P


EVERY = ("tp", "rep", "fs")
CHIPS = ("rep", "fs")
RING = 4
BF16, F32 = jnp.bfloat16, jnp.float32
ANY = pl.BlockSpec(memory_space=pl.ANY)
VMEM = pl.BlockSpec(memory_space=pltpu.VMEM)


def shift(x, axis, by):
    pairs = []
    for z in range(RING):
        for y in range(RING):
            for c in range(RING):
                to = [z, y, c]
                to[axis] = (to[axis] + by) % RING
                pairs.append(((z * RING + y) * RING + c, (to[0] * RING + to[1]) * RING + to[2]))
    return lax.ppermute(x, CHIPS, pairs)


def direct_ring(x, axis):
    return [x, shift(x, axis, 1), shift(x, axis, 2), shift(x, axis, 3)]


def passed_ring(x, axis, by):
    behind, ahead = shift(x, axis, 1), shift(x, axis, RING - 1)
    far = shift(behind if by == 1 else ahead, axis, by % RING)
    return [x, behind, far, ahead]


def relayed_ring(x, axis):
    half = x.shape[0] // 2
    behind, ahead = shift(x, axis, 1), shift(x, axis, RING - 1)
    return [x, behind, ahead, shift(behind[:half], axis, 1), shift(ahead[half:], axis, RING - 1)]


RELAYED = ((0, 0, 4, 0), (1, 0, 4, 1), (2, 0, 4, 3), (3, 0, 2, 2), (4, 2, 2, 2))


def in_place(pieces, position):
    out = []
    for j in range(RING):
        q = (position - j) % RING
        piece = pieces[0]
        for k in range(1, RING):
            piece = jnp.where(q == k, pieces[k], piece)
        out.append(piece)
    return jnp.stack(out)


def rms_scale(values, gain):
    values = values.astype(F32)
    scale = lax.rsqrt(jnp.mean(values * values, axis=-1, keepdims=True) + 1e-06)
    return values * scale * gain.astype(F32)


def dot_nn(a, b):
    return jnp.dot(a, b, preferred_element_type=F32)


def dot_nt(a, b):
    return lax.dot_general(a, b, (((1,), (1,)), ((), ())), preferred_element_type=F32)


def gelu(x):
    return 0.5 * x * (1.0 + jnp.tanh(0.7978845608028654 * (x + 0.044715 * (x * x * x))))


def mixer_body(own, *refs):
    normed_hbm = refs[0]
    for_unit, for_value, for_out = refs[1:6], refs[6:11], refs[11:16]
    mask_w, bias, gain, shifts, out, rows, w_unit, w_value, w_out, sem_x, sem_u, sem_v, sem_o = refs[16:]
    tp, rep, fs = lax.axis_index("tp"), lax.axis_index("rep"), lax.axis_index("fs")
    z, y, x_at = 2 * rep + fs // 16, fs // RING % RING, fs % RING
    count = rows.shape[0]
    start = pl.multiple_of((tp if own else 1 - tp) * count, count)
    pltpu.make_async_copy(normed_hbm.at[pl.ds(start, count)], rows, sem_x).start()
    part = w_unit.shape[3] // 2

    def line(ref, index, w, sem, at_z, at_y):
        to = pl.ds(pl.multiple_of(at_z // 2 * part, part), part)
        pltpu.make_async_copy(ref.at[index], w.at[at_z % 2, at_y, :, to], sem).start()

    def value_copies(piece, i, near, outer):
        line(for_value[piece], i, w_value, sem_v, (z + RING - near) % RING, (y + RING - outer) % RING)

    def unit_copies(piece, i, near, outer):
        line(for_unit[piece], i, w_unit, sem_u, (z + RING - outer) % RING, (y + RING - near) % RING)

    def out_copies(piece, i, near, outer):
        for r in range(2):
            pltpu.make_async_copy(
                for_out[piece].at[i, pl.ds(2 * r, 2)],
                w_out.at[:, (y + RING - near) % RING, (x_at + RING - outer) % RING, pl.ds(r * part, part)],
                sem_o,
            ).start()

    for start_copies in (value_copies, unit_copies, out_copies):
        for piece, low, inner, outer in RELAYED:

            def step(i, carry, piece=piece, low=low, outer=outer):
                start_copies(piece, i, low + i, outer)
                return carry

            lax.fori_loop(0, inner, step, 0)

    pltpu.make_async_copy(normed_hbm.at[pl.ds(start, count)], rows, sem_x).wait()
    pltpu.make_async_copy(w_value, w_value, sem_v).wait()
    x = rows[...]
    model, width = x.shape[1], w_value.shape[-1]
    value = gelu(dot_nn(x, w_value[...].reshape(model, width)))
    pltpu.make_async_copy(w_unit, w_unit, sem_u).wait()
    unit = gelu(dot_nn(x, w_unit[...].reshape(model, width)))
    groups, block = mask_w.shape[0], mask_w.shape[1]
    per = width // groups
    parts = []
    for g in range(groups):
        a = value[:, g * per : (g + 1) * per]
        a = a - jnp.mean(a, axis=-1, keepdims=True)
        a = a * lax.rsqrt(jnp.mean(a * a, axis=-1, keepdims=True) + 1e-06)
        a = a * gain[:, g * per : (g + 1) * per] + shifts[:, g * per : (g + 1) * per]
        a = a.astype(BF16)
        mixed = [
            dot_nn(mask_w[g], a[n * block : (n + 1) * block]) + bias[:, g : g + 1]
            for n in range(count // block)
        ]
        parts.append((unit[:, g * per : (g + 1) * per] * jnp.concatenate(mixed, axis=0)).astype(BF16))
    gated = jnp.concatenate(parts, axis=1)
    pltpu.make_async_copy(w_out, w_out, sem_o).wait()
    out[...] = dot_nt(gated, w_out[...].reshape(model, width)).astype(out.dtype)


def mixer(own, normed, pieces, mask_w, bias, gain, shifts, count, dtype):
    model, width = normed.shape[1], pieces[0].shape[-1]
    weight = pltpu.VMEM((2, RING, RING, model // 32, width), BF16)
    return pl.pallas_call(
        functools.partial(mixer_body, own),
        out_shape=jax.ShapeDtypeStruct((count, model), dtype),
        in_specs=[ANY] * 16 + [VMEM] * 4,
        out_specs=VMEM,
        scratch_shapes=[pltpu.VMEM((count, model), BF16), weight, weight, weight] + [pltpu.SemaphoreType.DMA] * 4,
        compiler_params=pltpu.CompilerParams(vmem_limit_bytes=56 * 2**20),
        name="mixer_own" if own else "mixer_other",
    )(normed, *pieces, mask_w, bias, gain, shifts)


CHUNK = 512


def ffn_body(h_hbm, n_hbm, packed, out_hbm, h_mid, normed, mid, down, hidden, out, sem_h, sem_n, sem_w, sem_d, sem_o):
    tps, share, wide = packed.shape[0], down.shape[2], packed.shape[-1]
    _, model = out.shape
    first = tps * wide % CHUNK
    starts = [0] * (first > 0) + list(range(first, tps * wide, CHUNK))
    sizes = [first] * (first > 0) + [CHUNK] * (tps * wide // CHUNK)

    def columns(j):
        copies = []
        for w in range(2):
            low, end = starts[j], starts[j] + sizes[j]
            while low < end:
                t = low // wide
                high = min(end, (t + 1) * wide)
                to = starts[j] + w * sizes[j] + low
                copies.append(
                    pltpu.make_async_copy(
                        packed.at[t, w, :, pl.ds(0, share), pl.ds(low - t * wide, high - low)],
                        mid.at[:, :, pl.ds(to, high - low)],
                        sem_w.at[j],
                    )
                )
                low = high
        return copies

    def downs(t):
        half = share // 2
        return [
            pltpu.make_async_copy(
                packed.at[t, r, :, pl.ds(share, half)], down.at[t, :, pl.ds(r * half, half)], sem_d
            )
            for r in range(2)
        ]

    rows = pltpu.make_async_copy(n_hbm, normed, sem_n)
    mids = pltpu.make_async_copy(h_hbm, h_mid, sem_h)
    for copy in columns(0):
        copy.start()
    rows.start()
    for j in range(1, len(sizes)):
        for copy in columns(j):
            copy.start()
    for t in range(tps):
        for copy in downs(t):
            copy.start()
    mids.start()
    rows.wait()

    def up_to(j, at, size):
        w = mid.at[:, :, pl.ds(2 * at, 2 * size)]
        pltpu.make_async_copy(w, w, sem_w.at[j]).wait()
        r = dot_nn(normed[...], w[...].reshape(model, 2 * size))
        hidden[:, pl.ds(at, size)] = (jax.nn.silu(r[:, :size]) * r[:, size:]).astype(BF16)

    for j, (at, size) in enumerate(zip(starts, sizes)):
        up_to(j, at, size)
    pltpu.make_async_copy(down, down, sem_d).wait()
    mids.wait()

    def leave(k):
        cols = pl.ds(pl.multiple_of(k * CHUNK, CHUNK), CHUNK)
        return pltpu.make_async_copy(out.at[:, cols], out_hbm.at[:, cols], sem_o.at[k])

    lines = CHUNK // share

    def back(k, carry):
        cols = pl.ds(pl.multiple_of(k * CHUNK, CHUNK), CHUNK)
        acc = h_mid[:, cols].astype(F32)
        for t in range(tps):
            w = down[t, pl.ds(k * lines, lines)].reshape(CHUNK, wide)
            acc = acc + dot_nt(hidden[:, t * wide : (t + 1) * wide], w)
        out[:, cols] = acc.astype(BF16)
        leave(k).start()
        return carry

    lax.fori_loop(0, model // CHUNK, back, 0)
    for k in range(model // CHUNK):
        leave(k).wait()


def ffn(h_mid, normed, packed, share):
    tps, _, fs, _, wide = packed.shape
    row = pltpu.VMEM(h_mid.shape, BF16)
    return pl.pallas_call(
        ffn_body,
        out_shape=jax.ShapeDtypeStruct(h_mid.shape, BF16),
        in_specs=[ANY] * 3,
        out_specs=ANY,
        scratch_shapes=[
            row, row, pltpu.VMEM((fs, share, 2 * tps * wide), BF16), pltpu.VMEM((tps, fs, share, wide), BF16),
            pltpu.VMEM((h_mid.shape[0], tps * wide), BF16), row,
            pltpu.SemaphoreType.DMA, pltpu.SemaphoreType.DMA, pltpu.SemaphoreType.DMA((-(-tps * wide // CHUNK),)),
            pltpu.SemaphoreType.DMA, pltpu.SemaphoreType.DMA((h_mid.shape[1] // CHUNK,)),
        ],
        compiler_params=pltpu.CompilerParams(vmem_limit_bytes=58 * 2**20),
        name="ffn",
    )(h_mid, normed, packed)


def pack_body(gate, up, down, out):
    rep = lax.axis_index("rep")
    share = gate.shape[0]
    half = share // 2
    out[:share] = jnp.where(rep == 0, gate[...], up[...])
    out[share:] = down[pl.ds(pl.multiple_of(rep * half, half), half)]


def pack(gate, up, down):
    share, wide = gate.shape
    return pl.pallas_call(
        pack_body,
        out_shape=jax.ShapeDtypeStruct((share + share // 2, wide), gate.dtype),
        in_specs=[VMEM] * 3,
        out_specs=VMEM,
        name="pack",
    )(gate, up, down)


def half_rows(x, part):
    size = x.shape[0] // 2
    return lax.dynamic_slice_in_dim(x, part * size, size, 0)


def on_device(
    tokens, norm_mix, w_unit, w_value, spatial, spatial_bias, group_gain, group_shift,
    w_mix_out, norm_ffn, w_gate, w_up, w_down,
):
    tp, rep, fs = (lax.axis_index(a) for a in ("tp", "rep", "fs"))
    tps, reps, fss = (lax.axis_size(a) for a in ("tp", "rep", "fs"))
    rows = tokens.shape[0] // tps
    share, width = w_unit.shape

    packed = pack(w_gate, w_up, w_down.T)
    packed = lax.all_gather(packed, EVERY).reshape(tps, reps, fss, *packed.shape)

    part = share // 2
    line = jnp.concatenate([half_rows(w_unit, rep), half_rows(w_value, rep)], axis=0)
    line = in_place(direct_ring(line, 2), fs % RING)
    for_unit = relayed_ring(jnp.stack(passed_ring(line[:, :part], 1, 1)), 0)
    for_value = relayed_ring(jnp.stack(passed_ring(line[:, part:], 0, 1)), 1)
    for_out = in_place(direct_ring(half_rows(w_mix_out.T, rep), 0), 2 * rep + fs // 16)
    for_out = relayed_ring(jnp.stack(passed_ring(for_out, 1, -1)), 2)

    groups = spatial.shape[0] // tps
    causal = jnp.tril(jnp.ones(spatial.shape[1:], dtype=bool))
    mask_w = lax.dynamic_slice_in_dim(jnp.where(causal[None], spatial, 0), tp * groups, groups, 0)
    bias = lax.dynamic_slice_in_dim(spatial_bias, tp * groups, groups, 0).astype(F32).T
    gain = lax.dynamic_slice_in_dim(group_gain, tp * width, width, 0).astype(F32)[None]
    shifts = lax.dynamic_slice_in_dim(group_shift, tp * width, width, 0).astype(F32)[None]
    normed = rms_scale(tokens, norm_mix).astype(BF16)

    unit = functools.partial(
        mixer, normed=normed, pieces=(*for_unit, *for_value, *for_out), mask_w=mask_w, bias=bias, gain=gain,
        shifts=shifts, count=rows,
    )
    other = unit(False, dtype=F32)
    arrived = lax.ppermute(other, "tp", [(i, (i + 1) % tps) for i in range(tps)])
    kept = unit(True, dtype=F32)
    residual = lax.dynamic_slice_in_dim(tokens, tp * rows, rows, 0).astype(F32)
    h_mid = (residual + (kept + arrived)).astype(BF16)
    normed_mid = rms_scale(h_mid, norm_ffn).astype(BF16)
    return ffn(h_mid, normed_mid, packed, share)


def solution(mesh):
    placed = (
        P(("rep", "fs"), None), P(), P("fs", "tp"), P("fs", "tp"), P(), P(), P(), P(),
        P("tp", "fs"), P(), P("fs", "tp"), P("fs", "tp"), P("tp", "fs"),
    )

    return jax.shard_map(on_device, mesh=mesh, in_specs=placed, out_specs=P(("rep", "fs", "tp"), None), check_vma=False)
```

```python
import functools

import jax
import jax.numpy as jnp
from jax import lax
from jax.experimental import pallas as pl
from jax.experimental.pallas import tpu as pltpu
from jax.sharding import PartitionSpec as P


EVERY = ("tp", "rep", "fs")
CHIPS = ("rep", "fs")
RING = 4
BF16, F32 = jnp.bfloat16, jnp.float32
ANY = pl.BlockSpec(memory_space=pl.ANY)
VMEM = pl.BlockSpec(memory_space=pltpu.VMEM)


def shift(x, axis, by):
    pairs = []
    for z in range(RING):
        for y in range(RING):
            for c in range(RING):
                to = [z, y, c]
                to[axis] = (to[axis] + by) % RING
                pairs.append(((z * RING + y) * RING + c, (to[0] * RING + to[1]) * RING + to[2]))
    return lax.ppermute(x, CHIPS, pairs)


def direct_ring(x, axis):
    return [x, shift(x, axis, 1), shift(x, axis, 2), shift(x, axis, 3)]


def passed_ring(x, axis, by):
    behind, ahead = shift(x, axis, 1), shift(x, axis, RING - 1)
    far = shift(behind if by == 1 else ahead, axis, by % RING)
    return [x, behind, far, ahead]


def relayed_ring(x, axis):
    half = x.shape[0] // 2
    behind, ahead = shift(x, axis, 1), shift(x, axis, RING - 1)
    return [x, behind, ahead, shift(behind[:half], axis, 1), shift(ahead[half:], axis, RING - 1)]


RELAYED = ((0, 0, 4, 0), (1, 0, 4, 1), (2, 0, 4, 3), (3, 0, 2, 2), (4, 2, 2, 2))


def in_place(pieces, position):
    out = []
    for j in range(RING):
        q = (position - j) % RING
        piece = pieces[0]
        for k in range(1, RING):
            piece = jnp.where(q == k, pieces[k], piece)
        out.append(piece)
    return jnp.stack(out)


def rms_scale(values, gain):
    values = values.astype(F32)
    scale = lax.rsqrt(jnp.mean(values * values, axis=-1, keepdims=True) + 1e-06)
    return values * scale * gain.astype(F32)


def dot_nn(a, b):
    return jnp.dot(a, b, preferred_element_type=F32)


def dot_nt(a, b):
    return lax.dot_general(a, b, (((1,), (1,)), ((), ())), preferred_element_type=F32)


def gelu(x):
    return 0.5 * x * (1.0 + jnp.tanh(0.7978845608028654 * (x + 0.044715 * (x * x * x))))


def mixer_body(own, *refs):
    normed_hbm = refs[0]
    for_unit, for_value, for_out = refs[1:6], refs[6:11], refs[11:16]
    mask_w, bias, gain, shifts, out, rows, w_unit, w_value, w_out, sem_x, sem_u, sem_v, sem_o = refs[16:]
    tp, rep, fs = lax.axis_index("tp"), lax.axis_index("rep"), lax.axis_index("fs")
    z, y, x_at = 2 * rep + fs // 16, fs // RING % RING, fs % RING
    count = rows.shape[0]
    start = pl.multiple_of((tp if own else 1 - tp) * count, count)
    pltpu.make_async_copy(normed_hbm.at[pl.ds(start, count)], rows, sem_x).start()
    part = w_unit.shape[3] // 2

    def line(ref, index, w, sem, at_z, at_y):
        to = pl.ds(pl.multiple_of(at_z // 2 * part, part), part)
        pltpu.make_async_copy(ref.at[index], w.at[at_z % 2, at_y, :, to], sem).start()

    def value_copies(piece, i, near, outer):
        line(for_value[piece], i, w_value, sem_v, (z + RING - near) % RING, (y + RING - outer) % RING)

    def unit_copies(piece, i, near, outer):
        line(for_unit[piece], i, w_unit, sem_u, (z + RING - outer) % RING, (y + RING - near) % RING)

    def out_copies(piece, i, near, outer):
        for r in range(2):
            pltpu.make_async_copy(
                for_out[piece].at[i, pl.ds(2 * r, 2)],
                w_out.at[:, (y + RING - near) % RING, (x_at + RING - outer) % RING, pl.ds(r * part, part)],
                sem_o,
            ).start()

    for start_copies in (value_copies, unit_copies, out_copies):
        for piece, low, inner, outer in RELAYED:

            def step(i, carry, piece=piece, low=low, outer=outer):
                start_copies(piece, i, low + i, outer)
                return carry

            lax.fori_loop(0, inner, step, 0)

    pltpu.make_async_copy(normed_hbm.at[pl.ds(start, count)], rows, sem_x).wait()
    pltpu.make_async_copy(w_value, w_value, sem_v).wait()
    x = rows[...]
    model, width = x.shape[1], w_value.shape[-1]
    value = gelu(dot_nn(x, w_value[...].reshape(model, width)))
    pltpu.make_async_copy(w_unit, w_unit, sem_u).wait()
    unit = gelu(dot_nn(x, w_unit[...].reshape(model, width)))
    groups, block = mask_w.shape[0], mask_w.shape[1]
    per = width // groups
    parts = []
    for g in range(groups):
        a = value[:, g * per : (g + 1) * per]
        a = a - jnp.mean(a, axis=-1, keepdims=True)
        a = a * lax.rsqrt(jnp.mean(a * a, axis=-1, keepdims=True) + 1e-06)
        a = a * gain[:, g * per : (g + 1) * per] + shifts[:, g * per : (g + 1) * per]
        a = a.astype(BF16)
        mixed = [
            dot_nn(mask_w[g], a[n * block : (n + 1) * block]) + bias[:, g : g + 1]
            for n in range(count // block)
        ]
        parts.append((unit[:, g * per : (g + 1) * per] * jnp.concatenate(mixed, axis=0)).astype(BF16))
    gated = jnp.concatenate(parts, axis=1)
    pltpu.make_async_copy(w_out, w_out, sem_o).wait()
    out[...] = dot_nt(gated, w_out[...].reshape(model, width)).astype(out.dtype)


def mixer(own, normed, pieces, mask_w, bias, gain, shifts, count, dtype):
    model, width = normed.shape[1], pieces[0].shape[-1]
    weight = pltpu.VMEM((2, RING, RING, model // 32, width), BF16)
    return pl.pallas_call(
        functools.partial(mixer_body, own),
        out_shape=jax.ShapeDtypeStruct((count, model), dtype),
        in_specs=[ANY] * 16 + [VMEM] * 4,
        out_specs=VMEM,
        scratch_shapes=[pltpu.VMEM((count, model), BF16), weight, weight, weight] + [pltpu.SemaphoreType.DMA] * 4,
        compiler_params=pltpu.CompilerParams(vmem_limit_bytes=56 * 2**20),
        name="mixer_own" if own else "mixer_other",
    )(normed, *pieces, mask_w, bias, gain, shifts)


CHUNK = 512


def ffn_body(h_hbm, n_hbm, packed, out_hbm, h_mid, normed, mid, down, hidden, out, sem_h, sem_n, sem_w, sem_d, sem_o):
    tps, share, wide = packed.shape[0], down.shape[1], packed.shape[-1]
    _, model = out.shape
    first = tps * wide % CHUNK
    starts = [0] * (first > 0) + list(range(first, tps * wide, CHUNK))
    sizes = [first] * (first > 0) + [CHUNK] * (tps * wide // CHUNK)

    def columns(j):
        copies = []
        for w in range(2):
            low, end = starts[j], starts[j] + sizes[j]
            while low < end:
                t = low // wide
                high = min(end, (t + 1) * wide)
                to = starts[j] + w * sizes[j] + low
                copies.append(
                    pltpu.make_async_copy(
                        packed.at[t, w, :, pl.ds(0, share), pl.ds(low - t * wide, high - low)],
                        mid.at[:, :, pl.ds(to, high - low)],
                        sem_w.at[j],
                    )
                )
                low = high
        return copies

    def downs(t):
        half = share // 2
        return [
            pltpu.make_async_copy(
                packed.at[t, r, :, pl.ds(share, half)], down.at[:, pl.ds(r * half, half), pl.ds(t * wide, wide)], sem_d
            )
            for r in range(2)
        ]

    rows = pltpu.make_async_copy(n_hbm, normed, sem_n)
    mids = pltpu.make_async_copy(h_hbm, h_mid, sem_h)
    for copy in columns(0):
        copy.start()
    rows.start()
    for j in range(1, len(sizes)):
        for copy in columns(j):
            copy.start()
    for t in range(tps):
        for copy in downs(t):
            copy.start()
    mids.start()
    rows.wait()

    def up_to(j, at, size):
        w = mid.at[:, :, pl.ds(2 * at, 2 * size)]
        pltpu.make_async_copy(w, w, sem_w.at[j]).wait()
        r = dot_nn(normed[...], w[...].reshape(model, 2 * size))
        hidden[:, pl.ds(at, size)] = (jax.nn.silu(r[:, :size]) * r[:, size:]).astype(BF16)

    if first:
        up_to(0, 0, first)

    def whole(j, carry):
        up_to(j + (first > 0), pl.multiple_of(first + j * CHUNK, 128), CHUNK)
        return carry

    lax.fori_loop(0, tps * wide // CHUNK, whole, 0)
    pltpu.make_async_copy(down, down, sem_d).wait()
    mids.wait()

    def leave(k):
        cols = pl.ds(k * CHUNK, CHUNK)
        return pltpu.make_async_copy(out.at[:, cols], out_hbm.at[:, cols], sem_o.at[k])

    lines = CHUNK // share

    for k in range(model // CHUNK):
        cols = slice(k * CHUNK, (k + 1) * CHUNK)
        w = down[k * lines : (k + 1) * lines].reshape(CHUNK, tps * wide)
        out[:, cols] = (h_mid[:, cols].astype(F32) + dot_nt(hidden[...], w)).astype(BF16)
        leave(k).start()
    for k in range(model // CHUNK):
        leave(k).wait()


def ffn(h_mid, normed, packed, share):
    tps, _, fs, _, wide = packed.shape
    row = pltpu.VMEM(h_mid.shape, BF16)
    return pl.pallas_call(
        ffn_body,
        out_shape=jax.ShapeDtypeStruct(h_mid.shape, BF16),
        in_specs=[ANY] * 3,
        out_specs=ANY,
        scratch_shapes=[
            row, row, pltpu.VMEM((fs, share, 2 * tps * wide), BF16), pltpu.VMEM((fs, share, tps * wide), BF16),
            pltpu.VMEM((h_mid.shape[0], tps * wide), BF16), row,
            pltpu.SemaphoreType.DMA, pltpu.SemaphoreType.DMA, pltpu.SemaphoreType.DMA((-(-tps * wide // CHUNK),)),
            pltpu.SemaphoreType.DMA, pltpu.SemaphoreType.DMA((h_mid.shape[1] // CHUNK,)),
        ],
        compiler_params=pltpu.CompilerParams(vmem_limit_bytes=58 * 2**20),
        name="ffn",
    )(h_mid, normed, packed)


def pack_body(gate, up, down, out):
    rep = lax.axis_index("rep")
    share = gate.shape[0]
    half = share // 2
    out[:share] = jnp.where(rep == 0, gate[...], up[...])
    out[share:] = down[pl.ds(pl.multiple_of(rep * half, half), half)]


def pack(gate, up, down):
    share, wide = gate.shape
    return pl.pallas_call(
        pack_body,
        out_shape=jax.ShapeDtypeStruct((share + share // 2, wide), gate.dtype),
        in_specs=[VMEM] * 3,
        out_specs=VMEM,
        name="pack",
    )(gate, up, down)


def half_rows(x, part):
    size = x.shape[0] // 2
    return lax.dynamic_slice_in_dim(x, part * size, size, 0)


def on_device(
    tokens, norm_mix, w_unit, w_value, spatial, spatial_bias, group_gain, group_shift,
    w_mix_out, norm_ffn, w_gate, w_up, w_down,
):
    tp, rep, fs = (lax.axis_index(a) for a in ("tp", "rep", "fs"))
    tps, reps, fss = (lax.axis_size(a) for a in ("tp", "rep", "fs"))
    rows = tokens.shape[0] // tps
    share, width = w_unit.shape

    packed = pack(w_gate, w_up, w_down.T)
    packed = lax.all_gather(packed, EVERY).reshape(tps, reps, fss, *packed.shape)

    part = share // 2
    line = jnp.concatenate([half_rows(w_unit, rep), half_rows(w_value, rep)], axis=0)
    line = in_place(direct_ring(line, 2), fs % RING)
    for_unit = relayed_ring(jnp.stack(passed_ring(line[:, :part], 1, 1)), 0)
    for_value = relayed_ring(jnp.stack(passed_ring(line[:, part:], 0, 1)), 1)
    for_out = in_place(direct_ring(half_rows(w_mix_out.T, rep), 0), 2 * rep + fs // 16)
    for_out = relayed_ring(jnp.stack(passed_ring(for_out, 1, -1)), 2)

    groups = spatial.shape[0] // tps
    causal = jnp.tril(jnp.ones(spatial.shape[1:], dtype=bool))
    mask_w = lax.dynamic_slice_in_dim(jnp.where(causal[None], spatial, 0), tp * groups, groups, 0)
    bias = lax.dynamic_slice_in_dim(spatial_bias, tp * groups, groups, 0).astype(F32).T
    gain = lax.dynamic_slice_in_dim(group_gain, tp * width, width, 0).astype(F32)[None]
    shifts = lax.dynamic_slice_in_dim(group_shift, tp * width, width, 0).astype(F32)[None]
    normed = rms_scale(tokens, norm_mix).astype(BF16)

    unit = functools.partial(
        mixer, normed=normed, pieces=(*for_unit, *for_value, *for_out), mask_w=mask_w, bias=bias, gain=gain,
        shifts=shifts, count=rows,
    )
    other = unit(False, dtype=F32)
    arrived = lax.ppermute(other, "tp", [(i, (i + 1) % tps) for i in range(tps)])
    kept = unit(True, dtype=F32)
    residual = lax.dynamic_slice_in_dim(tokens, tp * rows, rows, 0).astype(F32)
    h_mid = (residual + (kept + arrived)).astype(BF16)
    normed_mid = rms_scale(h_mid, norm_ffn).astype(BF16)
    return ffn(h_mid, normed_mid, packed, share)


def solution(mesh):
    placed = (
        P(("rep", "fs"), None), P(), P("fs", "tp"), P("fs", "tp"), P(), P(), P(), P(),
        P("tp", "fs"), P(), P("fs", "tp"), P("fs", "tp"), P("tp", "fs"),
    )

    return jax.shard_map(on_device, mesh=mesh, in_specs=placed, out_specs=P(("rep", "fs", "tp"), None), check_vma=False)
```
